32 devices in a mesh: sp: 8 (over z, core), tp: 4 (over y, x).
Axes of the slice: x: 2, y: 2, z: 4, core: 2. Of those that a mesh axis runs over, the one named last changes fastest.
Arguments:
- moe_in: bfloat16 [1536, 2048], P('sp'), may hold values from -6 to 6
- cotangent: bfloat16 [1536, 2048], P('sp'), may hold values from -6 to 6
- routing: int32 [1536, 2], P('sp'), may hold values from 0 to 7, as said below
- route_weight: float32 [1536, 2], P('sp'), may hold values from 0.2 to 1
- w_gate: bfloat16 [8, 2048, 2048], P('sp', 'tp'), may hold values from -0.125 to 0.125
- w_up: bfloat16 [8, 2048, 2048], P('sp', 'tp'), may hold values from -0.125 to 0.125
- w_down: bfloat16 [8, 2048, 2048], P('sp', 'tp'), may hold values from -0.125 to 0.125
- gate_b: bfloat16 [1024, 1536], P('tp', 'sp'), may hold values from -6 to 6
- gate_c: bfloat16 [1024, 1536], P('tp', 'sp'), may hold values from -6 to 6
- value_x: bfloat16 [1024, 1536], P('tp', 'sp'), may hold values from -6 to 6
- conv_taps: float32 [3, 1024], P(None, 'tp'), may hold values from -3 to 3
- out_proj: bfloat16 [1024, 2048], P('tp'), may hold values from -0.1875 to 0.1875
Outputs:
- w_gate_grad: bfloat16 [8, 2048, 2048], P('sp', 'tp')
- w_up_grad: bfloat16 [8, 2048, 2048], P('sp', 'tp')
- w_down_grad: bfloat16 [8, 2048, 2048], P('sp', 'tp')
- moe_in_grad: bfloat16 [1536, 2048], P('sp', 'tp')
- proj_grad: float32 [1024, 2048], P('tp', 'sp')
- gate_b_grad: bfloat16 [1024, 1536], P('tp', 'sp')
- gate_c_grad: bfloat16 [1024, 1536], P('tp', 'sp')
- value_x_grad: bfloat16 [1024, 1536], P('tp', 'sp')
The draws below stay inside these ranges and needn't reach their ends.
Inputs may be any that keep to these rules, and one draw needn't show every extreme that they name: `routing`: in each aligned block of 192 rows every expert is named exactly 48 times. The two entries of a row are different experts of one group; group g holds experts g * 2 to g * 2 + 1.
All inputs are finite; a program needn't handle non-finite values.
Results may differ from the reference program's by a relative error of at most 0.025.
Values may be sent and summed in bfloat16 or wider, within the bound.
A program may use at most 64 MiB of HBM per device.

```python
import jax
import jax.numpy as jnp
from jax import lax

D = 2048
W_A = 1024
HID = 2048
TAPS = 3
GROUPS = 4
TOPK = 2
TOK_DEV = 192
TOKENS = 1536
EXPERTS = 8
CAP = 48
HID_DEV = 512
N_SP = 8
N_TP = 4


def route_block(block_key):
    per_group = EXPERTS // GROUPS
    key_rank, key_shift, key_group, key_local = jax.random.split(block_key, 4)
    rank = jax.random.permutation(key_rank, TOK_DEV).astype(jnp.int32)
    first = rank % EXPERTS
    cycle = rank // EXPERTS
    offset = jax.random.randint(key_shift, (), 0, per_group, dtype=jnp.int32)
    shift = (cycle + offset) % max(per_group - 1, 1)
    group_id = first // per_group
    local_one = first % per_group
    local_two = (local_one + 1 + shift) % per_group
    group_perm = jax.random.permutation(key_group, GROUPS).astype(jnp.int32)
    local_perm = jax.random.permutation(key_local, per_group).astype(jnp.int32)
    expert_one = group_perm[group_id] * per_group + local_perm[local_one]
    expert_two = group_perm[group_id] * per_group + local_perm[local_two]
    return jnp.stack([expert_one, expert_two], axis=1)


def draw_routing(key, part):
    block_keys = jax.random.split(jax.random.fold_in(key, 17), TOKENS // TOK_DEV)
    blocks = jax.vmap(route_block)(block_keys)
    return blocks.reshape(TOKENS, TOPK).astype(jnp.int32)


def with_spikes(array, key, source, target, shards_of, factor):
    owner, partner = [(jnp.arange(array.shape[axis_at]) // (array.shape[axis_at] // shards_of)).reshape([-1 if axis == axis_at else 1 for axis in range(array.ndim)]) for axis_at in (source, target)]
    chosen = jax.random.permutation(key, shards_of)[partner]
    strong = (owner == chosen) | (owner == (partner + shards_of // 2) % shards_of)
    return jnp.where(strong, factor * array, array)


def block_scale(stream_key, shape, shards, smallest, top_value):
    loudness = 1.0
    for position, parts in shards:
        heights = jax.random.uniform(jax.random.fold_in(jax.random.fold_in(stream_key, 6), position), (parts,), jnp.float32, smallest / len(shards), top_value / len(shards))
        loudness = loudness * jnp.repeat(jnp.exp(heights), shape[position] // parts).reshape((-1,) + (1,) * (len(shape) - 1 - position))
    return loudness


def gaussian(stream_key, extent, scale, bound, cuts=(), kind=jnp.bfloat16):
    entries = scale * jax.random.normal(stream_key, extent, jnp.float32)
    if cuts:
        entries = entries * block_scale(stream_key, extent, cuts, -0.22, 0.18)
    return jnp.clip(entries, -bound, bound).astype(kind)


def gaussian_with(key, dims, deviation, most, cuts, heavy, kind=jnp.bfloat16):
    result = deviation * jax.random.normal(key, dims, jnp.float32)
    if cuts:
        result = result * block_scale(key, dims, cuts, -0.22, 0.18)
    return jnp.clip(with_spikes(result, jax.random.fold_in(key, 3), *heavy), -most, most).astype(kind)


def setup_inputs(seed: int = 0) -> dict:
    key_list = jax.random.split(jax.random.key(seed), 13)
    return {
        "moe_in": gaussian(key_list[0], (TOKENS, D), 1.0, 6.0, ((0, 8),)),
        "cotangent": gaussian_with(key_list[1], (TOKENS, D), 1.0, 6.0, ((0, 8),), (0, 1, 8, 2.0)),
        "routing": draw_routing(jax.random.fold_in(key_list[12], 71), 0),
        "route_weight": jnp.clip(0.2 + 0.8 * jax.random.uniform(key_list[3], (TOKENS, TOPK), jnp.float32) ** block_scale(key_list[3], (TOKENS, TOPK), ((0, 8),), -0.2, 0.2), 0.2, 1.0),
        "w_gate": gaussian(key_list[4], (EXPERTS, HID, D), D ** -0.5, 0.125, ((0, 8), (1, 4))),
        "w_up": gaussian(key_list[5], (EXPERTS, HID, D), D ** -0.5, 0.125, ((0, 8), (1, 4))),
        "w_down": gaussian(key_list[6], (EXPERTS, HID, D), HID ** -0.5, 0.125, ((0, 8), (1, 4))),
        "gate_b": gaussian(key_list[7], (W_A, TOKENS), 1.0, 6.0, ((0, 4), (1, 8))),
        "gate_c": gaussian(key_list[8], (W_A, TOKENS), 1.0, 6.0, ((0, 4), (1, 8))),
        "value_x": gaussian(key_list[9], (W_A, TOKENS), 1.0, 6.0, ((0, 4), (1, 8))),
        "conv_taps": gaussian(key_list[10], (TAPS, W_A), 0.6, 3.0, ((1, 4),), jnp.float32),
        "out_proj": gaussian(key_list[11], (W_A, D), W_A ** -0.5, 0.1875, ((0, 4),)),
    }


def reference(moe_in, cotangent, routing, route_weight, w_gate, w_up, w_down, gate_b, gate_c, value_x, conv_taps, out_proj):
    flat_routes = routing.reshape(-1)
    order = jnp.argsort(flat_routes, stable=True).astype(jnp.int32).reshape(EXPERTS, CAP * N_SP)
    weight_flat = route_weight.reshape(-1)
    contract_model = (((1,), (1,)), ((), ()))
    over_rows = (((0,), (0,)), ((), ()))

    def expert(packed):
        index, gate_weight, up_weight, down_weight = packed
        owner = index // TOPK
        arrived = moe_in[owner]
        route_cot = (weight_flat[index][:, None] * cotangent[owner].astype(jnp.float32)).astype(jnp.bfloat16)
        gate_pre = lax.dot_general(arrived, gate_weight, contract_model, preferred_element_type=jnp.float32)
        up_pre = lax.dot_general(arrived, up_weight, contract_model, preferred_element_type=jnp.float32)
        sigmoid_gate = jax.nn.sigmoid(gate_pre)
        hidden = (gate_pre * sigmoid_gate * up_pre).astype(jnp.bfloat16)
        hidden_grad = lax.dot_general(route_cot, down_weight, contract_model, preferred_element_type=jnp.float32)
        gate_grad = (hidden_grad * up_pre * sigmoid_gate * (1.0 + gate_pre * (1.0 - sigmoid_gate))).astype(jnp.bfloat16)
        up_grad = (hidden_grad * gate_pre * sigmoid_gate).astype(jnp.bfloat16)
        gate_wgrad = lax.dot_general(gate_grad, arrived, over_rows, preferred_element_type=jnp.float32).astype(jnp.bfloat16)
        up_wgrad = lax.dot_general(up_grad, arrived, over_rows, preferred_element_type=jnp.float32).astype(jnp.bfloat16)
        down_wgrad = lax.dot_general(hidden, route_cot, over_rows, preferred_element_type=jnp.float32).astype(jnp.bfloat16)
        row_total = gate_grad.shape[0]
        gate_blocks = gate_grad.astype(jnp.float32).reshape(row_total, N_TP, HID_DEV)
        up_blocks = up_grad.astype(jnp.float32).reshape(row_total, N_TP, HID_DEV)
        gate_table = gate_weight.astype(jnp.float32).reshape(N_TP, HID_DEV, D)
        up_table = up_weight.astype(jnp.float32).reshape(N_TP, HID_DEV, D)
        partial_value = jnp.einsum("rbh,bhd->brd", gate_blocks, gate_table) + jnp.einsum("rbh,bhd->brd", up_blocks, up_table)
        partial_value = lax.optimization_barrier(partial_value.astype(jnp.bfloat16)).astype(jnp.float32)
        route_grad = jnp.sum(partial_value, axis=0).astype(jnp.bfloat16)
        return gate_wgrad, up_wgrad, down_wgrad, route_grad

    w_gate_grad, w_up_grad, w_down_grad, route_grads = lax.map(expert, (order, w_gate, w_up, w_down))
    placed = jnp.zeros((TOKENS * TOPK, D), jnp.float32).at[order.reshape(-1)].set(route_grads.reshape(-1, D).astype(jnp.float32))
    moe_in_grad = jnp.sum(placed.reshape(TOKENS, TOPK, D), axis=1).astype(jnp.bfloat16)

    stream_grad = (cotangent.astype(jnp.float32) + moe_in_grad.astype(jnp.float32)).astype(jnp.bfloat16)
    mixed_in = lax.optimization_barrier((gate_c.astype(jnp.float32) * value_x.astype(jnp.float32)).astype(jnp.bfloat16))
    extended = jnp.pad(mixed_in.astype(jnp.float32), ((0, 0), (TAPS - 1, 0)))
    conv_out = jnp.zeros((W_A, TOKENS), jnp.float32)
    for tap in range(TAPS):
        conv_out = conv_out + conv_taps[tap][:, None] * extended[:, tap:tap + TOKENS]
    mixer_act = (gate_b.astype(jnp.float32) * conv_out).astype(jnp.bfloat16)
    act_grad = lax.dot_general(out_proj, stream_grad, contract_model, preferred_element_type=jnp.float32)
    proj_grad = jnp.dot(mixer_act, stream_grad, preferred_element_type=jnp.float32)
    gate_b_grad = (act_grad * conv_out).astype(jnp.bfloat16)
    conv_grad = act_grad * gate_b.astype(jnp.float32)
    extended_grad = jnp.pad(conv_grad, ((0, 0), (0, TAPS - 1)))
    mixed_grad = jnp.zeros((W_A, TOKENS), jnp.float32)
    for tap in range(TAPS):
        offset = TAPS - 1 - tap
        mixed_grad = mixed_grad + conv_taps[tap][:, None] * extended_grad[:, offset:offset + TOKENS]
    gate_c_grad = (mixed_grad * value_x.astype(jnp.float32)).astype(jnp.bfloat16)
    value_x_grad = (mixed_grad * gate_c.astype(jnp.float32)).astype(jnp.bfloat16)
    return (w_gate_grad, w_up_grad, w_down_grad, moe_in_grad, proj_grad, gate_b_grad, gate_c_grad, value_x_grad)
```

```python
import functools
import types

import jax
import jax.numpy as jnp
from jax import lax
from jax.experimental import pallas as pl
from jax.experimental.pallas import tpu as pltpu
from jax.sharding import PartitionSpec as P

TAPS = 3
GROUPS = 4
CORES = 2
MESH = pl.DeviceIdType.MESH


def place():
    s, t = lax.axis_index("sp"), lax.axis_index("tp")
    z, c = lax.div(s, CORES), lax.rem(s, CORES)
    x, y = lax.rem(t, 2), lax.div(t, 2)
    lanes = (t + 1 - 2 * x, t + 2 - 4 * y, 3 - t)
    return s, t, z, c, lanes


def span(index, width):
    return pl.ds(pl.multiple_of(index * width, width), width)


def remote(src, dst, send_sem, recv_sem, target):
    return pltpu.make_async_remote_copy(
        src_ref=src,
        dst_ref=dst,
        send_sem=send_sem,
        recv_sem=recv_sem,
        device_id=target,
        device_id_type=MESH,
    )


def half(quarter, side, width):
    return pl.ds(pl.multiple_of(quarter * width + side * (width // 2), width // 2), width // 2)


def from_behind(array, axis, by):
    count = lax.axis_size(axis)
    pairs = [(i, i + by) for i in range(count) if 0 <= i + by < count]
    return lax.ppermute(array, axis, pairs)


def on_device_general(
    moe_in,
    cotangent,
    routing,
    route_weight,
    w_gate,
    w_up,
    w_down,
    gate_b,
    gate_c,
    value_x,
    conv_taps,
    out_proj,
):
    tok_rows = routing.shape[0]
    top_routes = routing.shape[1]
    experts = lax.axis_size("sp")
    lane_count = lax.axis_size("tp")
    model_width = moe_in.shape[1]
    capacity = top_routes * tok_rows // experts
    flat_routes = routing.reshape(-1)
    route_count = flat_routes.shape[0]
    one_hot = (flat_routes[:, None] == jnp.arange(experts, dtype=jnp.int32)[None, :]).astype(
        jnp.int32
    )
    slot_rank = jnp.sum(jnp.cumsum(one_hot, axis=0) * one_hot, axis=1) - 1
    slot_index = flat_routes * capacity + slot_rank
    source = (
        jnp.zeros((route_count,), jnp.int32)
        .at[slot_index]
        .set(jnp.arange(route_count, dtype=jnp.int32))
    )
    owner_token = source // top_routes
    scales = route_weight.reshape(-1)[source][:, None]
    col_width = model_width // lane_count
    col_start = lax.axis_index("tp") * col_width
    rows_part = lax.dynamic_slice_in_dim(moe_in, col_start, col_width, 1)[owner_token]
    cot_slice = lax.dynamic_slice_in_dim(cotangent, col_start, col_width, 1)[owner_token]
    cot_part = (scales * cot_slice.astype(jnp.float32)).astype(jnp.bfloat16)
    moved = (
        lax.all_to_all(rows_part, "sp", split_axis=0, concat_axis=0, tiled=True),
        lax.all_to_all(cot_part, "sp", split_axis=0, concat_axis=0, tiled=True),
    )
    arrived, arrived_cot = (
        lax.all_gather(moved[0], "tp", axis=1, tiled=True),
        lax.all_gather(moved[1], "tp", axis=1, tiled=True),
    )
    contract_model = (((1,), (1,)), ((), ()))
    over_rows = (((0,), (0,)), ((), ()))
    gate_pre = lax.dot_general(
        arrived, w_gate[0], contract_model, preferred_element_type=jnp.float32
    )
    up_pre = lax.dot_general(arrived, w_up[0], contract_model, preferred_element_type=jnp.float32)
    sigmoid_gate = jax.nn.sigmoid(gate_pre)
    hidden = (gate_pre * sigmoid_gate * up_pre).astype(jnp.bfloat16)
    hidden_grad = lax.dot_general(
        arrived_cot, w_down[0], contract_model, preferred_element_type=jnp.float32
    )
    gate_grad = (
        hidden_grad * up_pre * sigmoid_gate * (1.0 + gate_pre * (1.0 - sigmoid_gate))
    ).astype(jnp.bfloat16)
    up_grad = (hidden_grad * gate_pre * sigmoid_gate).astype(jnp.bfloat16)
    w_gate_grad = lax.dot_general(
        gate_grad, arrived, over_rows, preferred_element_type=jnp.float32
    ).astype(jnp.bfloat16)[None]
    w_up_grad = lax.dot_general(
        up_grad, arrived, over_rows, preferred_element_type=jnp.float32
    ).astype(jnp.bfloat16)[None]
    w_down_grad = lax.dot_general(
        hidden, arrived_cot, over_rows, preferred_element_type=jnp.float32
    ).astype(jnp.bfloat16)[None]
    partial_value = jnp.dot(gate_grad, w_gate[0], preferred_element_type=jnp.float32) + jnp.dot(
        up_grad, w_up[0], preferred_element_type=jnp.float32
    )
    partial_value = lax.optimization_barrier(partial_value.astype(jnp.bfloat16)).astype(jnp.float32)
    summed = lax.psum_scatter(
        partial_value.astype(jnp.bfloat16), "tp", scatter_dimension=1, tiled=True
    )
    returned = lax.all_to_all(summed, "sp", split_axis=0, concat_axis=0, tiled=True)
    per_route = returned[slot_index].astype(jnp.float32)
    moe_in_grad = jnp.sum(per_route.reshape(tok_rows, top_routes, -1), axis=1).astype(jnp.bfloat16)
    full_grad = lax.all_gather(moe_in_grad, "tp", axis=1, tiled=True)
    stream_grad = (cotangent.astype(jnp.float32) + full_grad.astype(jnp.float32)).astype(
        jnp.bfloat16
    )
    mixed_in = lax.optimization_barrier(
        (gate_c.astype(jnp.float32) * value_x.astype(jnp.float32)).astype(jnp.bfloat16)
    )
    earlier = from_behind(mixed_in[:, tok_rows - (TAPS - 1) :], "sp", 1)
    extended = jnp.concatenate([earlier, mixed_in], axis=1).astype(jnp.float32)
    conv_out = jnp.zeros(mixed_in.shape, jnp.float32)
    for tap in range(TAPS):
        conv_out = conv_out + conv_taps[tap][:, None] * extended[:, tap : tap + tok_rows]
    mixer_act = (gate_b.astype(jnp.float32) * conv_out).astype(jnp.bfloat16)
    act_grad = lax.dot_general(
        out_proj, stream_grad, contract_model, preferred_element_type=jnp.float32
    )
    proj_rows = lax.psum_scatter(
        lax.dot_general(
            stream_grad, mixer_act, (((0,), (1,)), ((), ())), preferred_element_type=jnp.float32
        ).astype(jnp.bfloat16),
        "sp",
        scatter_dimension=0,
        tiled=True,
    ).astype(jnp.float32)
    proj_grad = proj_rows.T
    gate_b_grad = (act_grad * conv_out).astype(jnp.bfloat16)
    conv_grad = act_grad * gate_b.astype(jnp.float32)
    later = from_behind(conv_grad[:, : TAPS - 1], "sp", -1)
    extended_grad = jnp.concatenate([conv_grad, later], axis=1)
    mixed_grad = jnp.zeros(conv_grad.shape, jnp.float32)
    for tap in range(TAPS):
        offset = TAPS - 1 - tap
        mixed_grad = (
            mixed_grad + conv_taps[tap][:, None] * extended_grad[:, offset : offset + tok_rows]
        )
    gate_c_grad = (mixed_grad * value_x.astype(jnp.float32)).astype(jnp.bfloat16)
    value_x_grad = (mixed_grad * gate_c.astype(jnp.float32)).astype(jnp.bfloat16)
    return (
        w_gate_grad,
        w_up_grad,
        w_down_grad,
        moe_in_grad,
        proj_grad,
        gate_b_grad,
        gate_c_grad,
        value_x_grad,
    )


def last_dims(lhs, rhs):
    return lax.dot_general(lhs, rhs, (((1,), (1,)), ((), ())), preferred_element_type=jnp.float32)


def first_dims(lhs, rhs):
    return lax.dot_general(lhs, rhs, (((0,), (0,)), ((), ())), preferred_element_type=jnp.float32)


def plain(lhs, rhs):
    return jnp.dot(lhs, rhs, preferred_element_type=jnp.float32)


def step_kernel(names, *refs):
    r = types.SimpleNamespace(**dict(zip(names, refs)))
    s, t, z, c, lanes = place()
    tokens, model = r.moe.shape
    chan = r.gate_b.shape[1]
    cap = tokens // GROUPS
    width = model // 4
    hid_rows = r.w_gate.shape[0]
    devices = CORES * GROUPS
    f32, b16 = jnp.float32, jnp.bfloat16
    far = [z, z + 1 - 2 * lax.rem(z, 2), z + 2 - 4 * lax.div(z, 2), 3 - z]
    peer = [(CORES * far[d] + c, t) for d in range(GROUPS)]
    mate = (CORES * z + 1 - c, t)
    after, before = (lax.rem(s + 1, devices), t), (lax.rem(s + devices - 1, devices), t)
    side_z = lax.rem(z + GROUPS + 2 * c - 1, GROUPS)
    side = (CORES * side_z + 1 - c, t)
    lane = [(s, lanes[j]) for j in range(3)]
    mine = span(t, width)

    loads = {}
    order = ("moe", "cot", "gate_c", "value_x", "w_gate", "w_up", "w_down", "gate_b", "taps", "out_proj")
    for i, key in enumerate(order):
        loads[key] = pltpu.make_async_copy(getattr(r, key), getattr(r, "v_" + key), r.load.at[i])
        loads[key].start()
    targets = peer[1:] + [mate] + lane + [side]
    barrier = pltpu.get_barrier_semaphore()
    for target in targets:
        pl.semaphore_signal(barrier, inc=1, device_id=target, device_id_type=MESH)

    down = lax.broadcasted_iota(jnp.int32, (tokens, tokens), 0)
    along = lax.broadcasted_iota(jnp.int32, (tokens, tokens), 1)
    eye = down == along

    def column(row):
        return jnp.sum(jnp.where(eye, row, 0.0), axis=1, keepdims=True)

    lead = r.routing[0:1, :]
    group = lax.div(lead, CORES)
    low, high = lax.rem(group, 2), lax.div(group, 2)
    z_low, z_high = lax.rem(z, 2), lax.div(z, 2)
    slot = (low + z_low - 2 * low * z_low) + 2 * (high + z_high - 2 * high * z_high)
    slot = slot.astype(f32)
    earlier = (column(slot) == slot) & (down < along)
    rank = jnp.sum(jnp.where(earlier, 1.0, 0.0), axis=0, keepdims=True)
    at_row = slot * cap + rank
    at_col = column(at_row)
    select = (at_row == down.astype(f32)).astype(f32).astype(b16)
    unselect = (at_col == along.astype(f32)).astype(f32).astype(b16)
    is_even = lax.rem(lead, CORES) == 0
    by_core = [
        column(jnp.where(is_even, r.route_weight[k : k + 1, :], r.route_weight[1 - k : 2 - k, :]))
        for k in range(CORES)
    ]
    lane_at = lax.broadcasted_iota(jnp.int32, (tokens, 128), 1).astype(f32)
    row_at = lax.broadcasted_iota(jnp.int32, (8, 128), 0)
    for d in range(GROUPS):
        hit = at_col == lane_at + float(d * cap)
        picked = [jnp.sum(jnp.where(hit, by_core[k], 0.0), axis=0, keepdims=True) for k in range(CORES)]
        r.weights[d] = jnp.where(row_at == 0, picked[0], picked[1])
    for a, key in enumerate(("moe", "cot")):
        loads[key].wait()
        for n in range(4):
            cols = slice(n * width, (n + 1) * width)
            r.rows[a, :, :, cols] = (
                plain(select, getattr(r, "v_" + key)[:, cols]).astype(b16).reshape(GROUPS, cap, width)
            )
    for a in range(2):
        r.land[a, 0, c] = r.rows[a, 0]
    r.weight_in[0, c] = r.weights[0]
    loads["gate_c"].wait()
    loads["value_x"].wait()
    mixed = (r.v_gate_c[...].astype(f32) * r.v_value_x[...].astype(f32)).astype(b16).astype(f32)
    r.edge[...] = mixed[tokens - 8 :, :]
    pl.semaphore_wait(barrier, len(targets))

    steps = [(a, d) for d in range(1, GROUPS) for a in range(2)]
    copies = []

    def send(*args):
        copy = remote(*args)
        copy.start()
        copies.append(copy)
        return copy

    first, small = {}, {}
    for a, d in steps:
        first[a, d] = send(
            r.rows.at[a, d, :, mine],
            r.land.at[a, d, c, :, mine],
            r.sz.at[a, d - 1],
            r.rz.at[a, d - 1],
            peer[d],
        )
        if a == 0:
            small[d] = send(
                r.weights.at[d], r.weight_in.at[d, c], r.sw.at[d - 1], r.rw.at[d - 1], peer[d]
            )
    fourth, small_mate = {}, {}
    for a in range(2):
        fourth[a, 0] = send(
            r.rows.at[a, 0], r.land.at[a, 0, c], r.sm.at[a, 0], r.rm.at[a, 0], mate
        )
    small_mate[0] = send(
        r.weights.at[0], r.weight_in.at[0, c], r.sv.at[0], r.rv.at[0], mate
    )
    halo = send(r.edge, r.edge_in, r.sh.at[0], r.rh.at[0], after)

    second, third = {}, {}

    def e1(a, d):
        first[a, d].wait_recv()
        block = r.land.at[a, d, c, :, mine]
        for j in range(2):
            second[a, d, j] = send(block, block, r.sx.at[a, d - 1, j], r.rx.at[a, d - 1, j], lane[j])
        if a == 0:
            small[d].wait_recv()
            block = r.weight_in.at[d, c]
            small_mate[d] = send(block, block, r.sv.at[d], r.rv.at[d], mate)

    def e2(a, d):
        for j in range(2):
            second[a, d, j].wait_recv()
        for j in range(2):
            block = r.land.at[a, d, c, :, half(lanes[1 - j], j, width)]
            third[a, d, j] = send(block, block, r.sy.at[a, d - 1, j], r.ry.at[a, d - 1, j], lane[j])

    def e3(a, d):
        for j in range(2):
            third[a, d, j].wait_recv()
        block = r.land.at[a, d, c]
        fourth[a, d] = send(block, block, r.sm.at[a, d], r.rm.at[a, d], mate)

    def e4(a, d):
        fourth[a, d].wait_recv()

    cap_down = lax.broadcasted_iota(jnp.int32, (cap, 128), 0)
    cap_along = lax.broadcasted_iota(jnp.int32, (cap, 128), 1)

    def forward(d):
        small_mate[d].wait_recv()
        for k in range(CORES):
            tile = r.weight_in[d, k]
            row = jnp.sum(jnp.where(row_at == c, tile, 0.0), axis=0, keepdims=True)
            scale = jnp.sum(jnp.where(cap_down == cap_along, row, 0.0), axis=1, keepdims=True)
            r.scaled[d, k] = (scale * r.land[1, d, k].astype(f32)).astype(b16)
        x = r.land[0, d].reshape(CORES * cap, model)
        y = r.scaled[d].reshape(CORES * cap, model)
        for n in range(hid_rows // 256):
            hs = slice(n * 256, (n + 1) * 256)
            gate = last_dims(x, r.v_w_gate[hs, :])
            up = last_dims(x, r.v_w_up[hs, :])
            grad = last_dims(y, r.v_w_down[hs, :])
            sig = jax.nn.sigmoid(gate)
            silu = gate * sig
            r.hidden[d, :, hs] = (silu * up).astype(b16)
            r.gate_grad[d, :, hs] = (grad * up * sig * (1.0 + gate * (1.0 - sig))).astype(b16)
            r.up_grad[d, :, hs] = (grad * silu).astype(b16)

    swap, across, home, spread, relay = {}, {}, {}, {}, {}

    def backward(d):
        for n in range(4):
            cols = slice(n * width, (n + 1) * width)
            value = plain(r.gate_grad[d], r.v_w_gate[:, cols]) + plain(
                r.up_grad[d], r.v_w_up[:, cols]
            )
            r.part[d, :, :, cols] = value.astype(b16).reshape(CORES, cap, width)
        swap[d] = send(r.part.at[d, 1 - c], r.mate_in.at[d], r.sa.at[d], r.ra.at[d], mate)

    def reduce_start(d):
        swap[d].wait_recv()
        r.total[d] = (r.part[d, c].astype(f32) + r.mate_in[d].astype(f32)).astype(b16)
        for j in (2, 0, 1):
            across[d, j] = send(
                r.total.at[d, :, span(lanes[j], width)],
                r.lane_in.at[d, j],
                r.sb.at[d, j],
                r.rb.at[d, j],
                lane[j],
            )

    def spread_start(d):
        block = r.home.at[d, :, mine]
        for j in range(2):
            spread[d, j] = send(block, block, r.sd.at[d, j], r.rd.at[d, j], lane[j])

    def reduce_end(d):
        value = r.total[d, :, mine].astype(f32)
        for j in range(3):
            across[d, j].wait_recv()
            value = value + r.lane_in[d, j].astype(f32)
        if d == 0:
            r.home[0, :, mine] = value.astype(b16)
            spread_start(0)
        else:
            r.done[d - 1] = value.astype(b16)
            home[d] = send(
                r.done.at[d - 1], r.home.at[d, :, mine], r.sc.at[d - 1], r.rc.at[d - 1], peer[d]
            )

    def home_in(d):
        home[d].wait_recv()
        spread_start(d)

    def relay_start(d):
        for j in range(2):
            spread[d, j].wait_recv()
        for j in range(2):
            block = r.home.at[d, :, half(lanes[1 - j], j, width)]
            relay[d, j] = send(block, block, r.se.at[d, j], r.re.at[d, j], lane[j])

    def relay_end(d):
        for j in range(2):
            relay[d, j].wait_recv()

    sources = (("w_gate_grad", "gate_grad", 0), ("w_up_grad", "up_grad", 0), ("w_down_grad", "hidden", 1))

    def weight_grad(i):
        out, left, a = sources[i]
        lhs = getattr(r, left)[...].reshape(GROUPS * CORES * cap, hid_rows)
        for n in range(4):
            cols = slice(n * width, (n + 1) * width)
            rhs = r.land[0, :, :, :, cols] if a == 0 else r.scaled[:, :, :, cols]
            getattr(r, out)[:, cols] = first_dims(lhs, rhs.reshape(GROUPS * CORES * cap, width)).astype(b16)

    token_at = lax.broadcasted_iota(jnp.int32, (tokens, chan), 0)

    def conv_forward():
        halo.wait_recv()
        loads["taps"].wait()
        loads["gate_b"].wait()
        keep = jnp.where(s == 0, 0.0, 1.0)
        one, two = keep * r.edge_in[7:8, :], keep * r.edge_in[6:7, :]
        back_one = jnp.where(token_at == 0, one, pltpu.roll(mixed, 1, 0))
        back_two = jnp.where(
            token_at == 0, two, jnp.where(token_at == 1, one, pltpu.roll(mixed, 2, 0))
        )
        taps = r.v_taps
        conv = taps[0:1, :] * back_two + taps[1:2, :] * back_one + taps[2:3, :] * mixed
        r.conv[...] = conv
        act = (r.v_gate_b[...].astype(f32) * conv).astype(b16)
        unit = lax.broadcasted_iota(jnp.int32, (chan, chan), 0) == lax.broadcasted_iota(
            jnp.int32, (chan, chan), 1
        )
        r.act[...] = last_dims(unit.astype(f32).astype(b16), act).astype(b16)

    for key in ("w_gate", "w_up", "w_down"):
        loads[key].wait()
    e4(0, 0)
    e4(1, 0)
    forward(0)
    backward(0)
    e1(*steps[0])
    e1(*steps[1])
    reduce_start(0)
    e2(*steps[0])
    e1(*steps[2])
    e2(*steps[1])
    e3(*steps[0])
    conv_forward()
    e1(*steps[3])
    e2(*steps[2])
    e3(*steps[1])
    e4(*steps[0])
    e4(*steps[1])
    forward(1)
    e1(*steps[4])
    e2(*steps[3])
    e3(*steps[2])
    backward(1)
    e1(*steps[5])
    reduce_end(0)
    e2(*steps[4])
    e3(*steps[3])
    e4(*steps[2])
    e4(*steps[3])
    reduce_start(1)
    forward(2)
    e2(*steps[5])
    e3(*steps[4])
    backward(2)
    e3(*steps[5])
    reduce_start(2)
    e4(*steps[4])
    e4(*steps[5])
    forward(3)
    reduce_end(1)
    backward(3)
    relay_start(0)
    reduce_start(3)
    reduce_end(2)
    weight_grad(0)
    home_in(1)
    reduce_end(3)
    home_in(2)
    relay_start(1)
    weight_grad(1)
    home_in(3)
    relay_start(2)
    weight_grad(2)
    relay_start(3)
    loads["out_proj"].wait()
    for d in range(GROUPS):
        relay_end(d)

    for n in range(4):
        cols = slice(n * width, (n + 1) * width)
        full = plain(unselect, r.home[:, :, cols].reshape(tokens, width)).astype(b16)
        r.full[:, cols] = full
        r.stream[:, cols] = (r.v_cot[:, cols].astype(f32) + full.astype(f32)).astype(b16)
    narrow = width // CORES
    pair = {}
    act = r.act[...]
    for d in (2, 3, 1, 0):
        cols = span(CORES * far[d] + 1 - c, narrow)
        r.give[d] = plain(act, r.stream[:, cols]).astype(b16)
        pair[d] = send(r.give.at[d], r.take.at[d], r.sp.at[d], r.rp.at[d], mate)
    act_grad = last_dims(r.stream[...], r.v_out_proj[...])
    conv_grad = act_grad * r.v_gate_b[...].astype(f32)
    r.rim[...] = conv_grad[0:8, :]
    rim = send(r.rim, r.rim_in, r.sh.at[1], r.rh.at[1], before)
    wide = {}
    near = None
    for d in (2, 3, 1, 0):
        cols = span(CORES * far[d] + c, narrow)
        value = plain(act, r.stream[:, cols])
        pair[d].wait_recv()
        value = value + r.take[d].astype(f32)
        if d == 0:
            near = value
        else:
            r.sum[d - 1] = value.astype(b16)
            wide[d] = send(
                r.sum.at[d - 1], r.wide_in.at[d - 1], r.sq.at[d - 1], r.rq.at[d - 1], peer[d]
            )
    r.moe_in_grad[...] = r.full[:, mine]
    r.gate_b_grad[...] = (act_grad * r.conv[...]).astype(b16)
    rim.wait_recv()
    keep = jnp.where(s == devices - 1, 0.0, 1.0)
    one, two = keep * r.rim_in[0:1, :], keep * r.rim_in[1:2, :]
    next_one = jnp.where(token_at == tokens - 1, one, pltpu.roll(conv_grad, tokens - 1, 0))
    next_two = jnp.where(
        token_at == tokens - 1,
        two,
        jnp.where(token_at == tokens - 2, one, pltpu.roll(conv_grad, tokens - 2, 0)),
    )
    taps = r.v_taps
    mixed_grad = taps[0:1, :] * next_two + taps[1:2, :] * next_one + taps[2:3, :] * conv_grad
    r.gate_c_grad[...] = (mixed_grad * r.v_value_x[...].astype(f32)).astype(b16)
    r.value_x_grad[...] = (mixed_grad * r.v_gate_c[...].astype(f32)).astype(b16)
    for d in (1, 2, 3):
        wide[d].wait_recv()
        near = near + r.wide_in[d - 1].astype(f32)
    r.proj_grad[...] = near
    for copy in copies:
        copy.wait_send()


def store_kernel(*refs):
    count = len(refs) // 2
    copies = [pltpu.make_async_copy(refs[i], refs[count + i], refs[-1].at[i]) for i in range(count)]
    for copy in copies:
        copy.start()
    for copy in copies:
        copy.wait()


def on_device_paired(
    moe_in, cotangent, routing, route_weight, w_gate, w_up, w_down, gate_b, gate_c, value_x, conv_taps, out_proj
):
    tokens, model = moe_in.shape
    hid_rows = w_gate.shape[1]
    chan = gate_b.shape[0]
    cap, width = tokens // GROUPS, model // 4
    b16, f32 = moe_in.dtype, jnp.float32
    vmem, hbm = pl.BlockSpec(memory_space=pltpu.VMEM), pl.BlockSpec(memory_space=pltpu.HBM)
    dma = pltpu.SemaphoreType.DMA
    inputs = dict(
        routing=routing.T,
        route_weight=route_weight.T,
        moe=moe_in,
        cot=cotangent,
        w_gate=w_gate[0],
        w_up=w_up[0],
        w_down=w_down[0],
        gate_b=gate_b.T,
        gate_c=gate_c.T,
        value_x=value_x.T,
        taps=conv_taps,
        out_proj=out_proj,
    )
    outputs = dict(
        w_gate_grad=((hid_rows, model), b16),
        w_up_grad=((hid_rows, model), b16),
        w_down_grad=((hid_rows, model), b16),
        moe_in_grad=((tokens, width), b16),
        proj_grad=((chan, width // CORES), f32),
        gate_b_grad=((tokens, chan), b16),
        gate_c_grad=((tokens, chan), b16),
        value_x_grad=((tokens, chan), b16),
    )
    loaded = [key for key in inputs if key not in ("routing", "route_weight")]
    scratch = {"v_" + key: pltpu.VMEM(inputs[key].shape, inputs[key].dtype) for key in loaded}
    three, pair = GROUPS - 1, CORES * cap
    scratch |= dict(
        weights=pltpu.VMEM((GROUPS, 8, 128), f32),
        weight_in=pltpu.VMEM((GROUPS, CORES, 8, 128), f32),
        rows=pltpu.VMEM((2, GROUPS, cap, model), b16),
        land=pltpu.VMEM((2, GROUPS, CORES, cap, model), b16),
        scaled=pltpu.VMEM((GROUPS, CORES, cap, model), b16),
        hidden=pltpu.VMEM((GROUPS, pair, hid_rows), b16),
        gate_grad=pltpu.VMEM((GROUPS, pair, hid_rows), b16),
        up_grad=pltpu.VMEM((GROUPS, pair, hid_rows), b16),
        part=pltpu.VMEM((GROUPS, CORES, cap, model), b16),
        mate_in=pltpu.VMEM((GROUPS, cap, model), b16),
        total=pltpu.VMEM((GROUPS, cap, model), b16),
        lane_in=pltpu.VMEM((GROUPS, 3, cap, width), b16),
        done=pltpu.VMEM((three, cap, width), b16),
        home=pltpu.VMEM((GROUPS, cap, model), b16),
        full=pltpu.VMEM((tokens, model), b16),
        stream=pltpu.VMEM((tokens, model), b16),
        conv=pltpu.VMEM((tokens, chan), f32),
        act=pltpu.VMEM((chan, tokens), b16),
        edge=pltpu.VMEM((8, chan), f32),
        edge_in=pltpu.VMEM((8, chan), f32),
        rim=pltpu.VMEM((8, chan), f32),
        rim_in=pltpu.VMEM((8, chan), f32),
        give=pltpu.VMEM((GROUPS, chan, width // CORES), b16),
        take=pltpu.VMEM((GROUPS, chan, width // CORES), b16),
        sum=pltpu.VMEM((three, chan, width // CORES), b16),
        wide_in=pltpu.VMEM((three, chan, width // CORES), b16),
        load=dma((len(loaded),)),
    )
    counts = dict(
        z=(2, three),
        w=(three,),
        x=(2, three, 2),
        y=(2, three, 2),
        m=(2, GROUPS),
        v=(GROUPS,),
        h=(2,),
        a=(GROUPS,),
        b=(GROUPS, 3),
        c=(three,),
        d=(GROUPS, 2),
        e=(GROUPS, 2),
        p=(GROUPS,),
        q=(three,),
    )
    for key, shape in counts.items():
        scratch["s" + key] = dma(shape)
        scratch["r" + key] = dma(shape)
    names = list(inputs) + list(outputs) + list(scratch)
    out = pl.pallas_call(
        functools.partial(step_kernel, names),
        out_shape=tuple(pltpu.VMEM(*shape) for shape in outputs.values()),
        in_specs=[hbm if key in loaded else vmem for key in inputs],
        out_specs=(vmem,) * len(outputs),
        scratch_shapes=list(scratch.values()),
        compiler_params=pltpu.CompilerParams(
            collective_id=0, has_side_effects=True, vmem_limit_bytes=54 * 1024 * 1024
        ),
        name="step",
    )(*inputs.values())
    out = pl.pallas_call(
        store_kernel,
        out_shape=tuple(jax.ShapeDtypeStruct(*shape) for shape in outputs.values()),
        in_specs=[vmem] * len(outputs),
        out_specs=(hbm,) * len(outputs),
        scratch_shapes=[dma((len(outputs),))],
        compiler_params=pltpu.CompilerParams(vmem_limit_bytes=4 * 1024 * 1024),
        name="store",
    )(*out)
    out = types.SimpleNamespace(**dict(zip(outputs, out)))
    return (
        out.w_gate_grad[None],
        out.w_up_grad[None],
        out.w_down_grad[None],
        out.moe_in_grad,
        out.proj_grad,
        out.gate_b_grad.T,
        out.gate_c_grad.T,
        out.value_x_grad.T,
    )


def on_device(*args):
    routes = args[2].shape[1]
    experts, lane_count = lax.axis_size("sp"), lax.axis_size("tp")
    if experts == CORES * GROUPS and routes == CORES and lane_count == 4:
        return on_device_paired(*args)
    return on_device_general(*args)


def solution(mesh):
    in_specs = (
        P("sp", None),
        P("sp", None),
        P("sp", None),
        P("sp", None),
        P("sp", "tp", None),
        P("sp", "tp", None),
        P("sp", "tp", None),
        P("tp", "sp"),
        P("tp", "sp"),
        P("tp", "sp"),
        P(None, "tp"),
        P("tp", None),
    )
    out_specs = (
        P("sp", "tp", None),
        P("sp", "tp", None),
        P("sp", "tp", None),
        P("sp", "tp"),
        P("tp", "sp"),
        P("tp", "sp"),
        P("tp", "sp"),
        P("tp", "sp"),
    )
    return jax.shard_map(
        on_device, mesh=mesh, in_specs=in_specs, out_specs=out_specs, check_vma=False
    )
```

```python
import functools
import types

import jax
import jax.numpy as jnp
from jax import lax
from jax.experimental import pallas as pl
from jax.experimental.pallas import tpu as pltpu
from jax.sharding import PartitionSpec as P

TAPS = 3
GROUPS = 4
CORES = 2
MESH = pl.DeviceIdType.MESH


def place():
    s, t = lax.axis_index("sp"), lax.axis_index("tp")
    z, c = lax.div(s, CORES), lax.rem(s, CORES)
    x, y = lax.rem(t, 2), lax.div(t, 2)
    lanes = (t + 1 - 2 * x, t + 2 - 4 * y, 3 - t)
    return s, t, z, c, lanes


def span(index, width):
    return pl.ds(pl.multiple_of(index * width, width), width)


def remote(src, dst, send_sem, recv_sem, target):
    return pltpu.make_async_remote_copy(
        src_ref=src,
        dst_ref=dst,
        send_sem=send_sem,
        recv_sem=recv_sem,
        device_id=target,
        device_id_type=MESH,
    )


def half(quarter, side, width):
    return pl.ds(pl.multiple_of(quarter * width + side * (width // 2), width // 2), width // 2)


def from_behind(array, axis, by):
    count = lax.axis_size(axis)
    pairs = [(i, i + by) for i in range(count) if 0 <= i + by < count]
    return lax.ppermute(array, axis, pairs)


def on_device_general(
    moe_in,
    cotangent,
    routing,
    route_weight,
    w_gate,
    w_up,
    w_down,
    gate_b,
    gate_c,
    value_x,
    conv_taps,
    out_proj,
):
    tok_rows = routing.shape[0]
    top_routes = routing.shape[1]
    experts = lax.axis_size("sp")
    lane_count = lax.axis_size("tp")
    model_width = moe_in.shape[1]
    capacity = top_routes * tok_rows // experts
    flat_routes = routing.reshape(-1)
    route_count = flat_routes.shape[0]
    one_hot = (flat_routes[:, None] == jnp.arange(experts, dtype=jnp.int32)[None, :]).astype(
        jnp.int32
    )
    slot_rank = jnp.sum(jnp.cumsum(one_hot, axis=0) * one_hot, axis=1) - 1
    slot_index = flat_routes * capacity + slot_rank
    source = (
        jnp.zeros((route_count,), jnp.int32)
        .at[slot_index]
        .set(jnp.arange(route_count, dtype=jnp.int32))
    )
    owner_token = source // top_routes
    scales = route_weight.reshape(-1)[source][:, None]
    col_width = model_width // lane_count
    col_start = lax.axis_index("tp") * col_width
    rows_part = lax.dynamic_slice_in_dim(moe_in, col_start, col_width, 1)[owner_token]
    cot_slice = lax.dynamic_slice_in_dim(cotangent, col_start, col_width, 1)[owner_token]
    cot_part = (scales * cot_slice.astype(jnp.float32)).astype(jnp.bfloat16)
    moved = (
        lax.all_to_all(rows_part, "sp", split_axis=0, concat_axis=0, tiled=True),
        lax.all_to_all(cot_part, "sp", split_axis=0, concat_axis=0, tiled=True),
    )
    arrived, arrived_cot = (
        lax.all_gather(moved[0], "tp", axis=1, tiled=True),
        lax.all_gather(moved[1], "tp", axis=1, tiled=True),
    )
    contract_model = (((1,), (1,)), ((), ()))
    over_rows = (((0,), (0,)), ((), ()))
    gate_pre = lax.dot_general(
        arrived, w_gate[0], contract_model, preferred_element_type=jnp.float32
    )
    up_pre = lax.dot_general(arrived, w_up[0], contract_model, preferred_element_type=jnp.float32)
    sigmoid_gate = jax.nn.sigmoid(gate_pre)
    hidden = (gate_pre * sigmoid_gate * up_pre).astype(jnp.bfloat16)
    hidden_grad = lax.dot_general(
        arrived_cot, w_down[0], contract_model, preferred_element_type=jnp.float32
    )
    gate_grad = (
        hidden_grad * up_pre * sigmoid_gate * (1.0 + gate_pre * (1.0 - sigmoid_gate))
    ).astype(jnp.bfloat16)
    up_grad = (hidden_grad * gate_pre * sigmoid_gate).astype(jnp.bfloat16)
    w_gate_grad = lax.dot_general(
        gate_grad, arrived, over_rows, preferred_element_type=jnp.float32
    ).astype(jnp.bfloat16)[None]
    w_up_grad = lax.dot_general(
        up_grad, arrived, over_rows, preferred_element_type=jnp.float32
    ).astype(jnp.bfloat16)[None]
    w_down_grad = lax.dot_general(
        hidden, arrived_cot, over_rows, preferred_element_type=jnp.float32
    ).astype(jnp.bfloat16)[None]
    partial_value = jnp.dot(gate_grad, w_gate[0], preferred_element_type=jnp.float32) + jnp.dot(
        up_grad, w_up[0], preferred_element_type=jnp.float32
    )
    partial_value = lax.optimization_barrier(partial_value.astype(jnp.bfloat16)).astype(jnp.float32)
    summed = lax.psum_scatter(
        partial_value.astype(jnp.bfloat16), "tp", scatter_dimension=1, tiled=True
    )
    returned = lax.all_to_all(summed, "sp", split_axis=0, concat_axis=0, tiled=True)
    per_route = returned[slot_index].astype(jnp.float32)
    moe_in_grad = jnp.sum(per_route.reshape(tok_rows, top_routes, -1), axis=1).astype(jnp.bfloat16)
    full_grad = lax.all_gather(moe_in_grad, "tp", axis=1, tiled=True)
    stream_grad = (cotangent.astype(jnp.float32) + full_grad.astype(jnp.float32)).astype(
        jnp.bfloat16
    )
    mixed_in = lax.optimization_barrier(
        (gate_c.astype(jnp.float32) * value_x.astype(jnp.float32)).astype(jnp.bfloat16)
    )
    earlier = from_behind(mixed_in[:, tok_rows - (TAPS - 1) :], "sp", 1)
    extended = jnp.concatenate([earlier, mixed_in], axis=1).astype(jnp.float32)
    conv_out = jnp.zeros(mixed_in.shape, jnp.float32)
    for tap in range(TAPS):
        conv_out = conv_out + conv_taps[tap][:, None] * extended[:, tap : tap + tok_rows]
    mixer_act = (gate_b.astype(jnp.float32) * conv_out).astype(jnp.bfloat16)
    act_grad = lax.dot_general(
        out_proj, stream_grad, contract_model, preferred_element_type=jnp.float32
    )
    proj_rows = lax.psum_scatter(
        lax.dot_general(
            stream_grad, mixer_act, (((0,), (1,)), ((), ())), preferred_element_type=jnp.float32
        ).astype(jnp.bfloat16),
        "sp",
        scatter_dimension=0,
        tiled=True,
    ).astype(jnp.float32)
    proj_grad = proj_rows.T
    gate_b_grad = (act_grad * conv_out).astype(jnp.bfloat16)
    conv_grad = act_grad * gate_b.astype(jnp.float32)
    later = from_behind(conv_grad[:, : TAPS - 1], "sp", -1)
    extended_grad = jnp.concatenate([conv_grad, later], axis=1)
    mixed_grad = jnp.zeros(conv_grad.shape, jnp.float32)
    for tap in range(TAPS):
        offset = TAPS - 1 - tap
        mixed_grad = (
            mixed_grad + conv_taps[tap][:, None] * extended_grad[:, offset : offset + tok_rows]
        )
    gate_c_grad = (mixed_grad * value_x.astype(jnp.float32)).astype(jnp.bfloat16)
    value_x_grad = (mixed_grad * gate_c.astype(jnp.float32)).astype(jnp.bfloat16)
    return (
        w_gate_grad,
        w_up_grad,
        w_down_grad,
        moe_in_grad,
        proj_grad,
        gate_b_grad,
        gate_c_grad,
        value_x_grad,
    )


def last_dims(lhs, rhs):
    return lax.dot_general(lhs, rhs, (((1,), (1,)), ((), ())), preferred_element_type=jnp.float32)


def first_dims(lhs, rhs):
    return lax.dot_general(lhs, rhs, (((0,), (0,)), ((), ())), preferred_element_type=jnp.float32)


def plain(lhs, rhs):
    return jnp.dot(lhs, rhs, preferred_element_type=jnp.float32)


def step_kernel(names, *refs):
    r = types.SimpleNamespace(**dict(zip(names, refs)))
    s, t, z, c, lanes = place()
    tokens, model = r.moe.shape
    chan = r.gate_b.shape[1]
    cap = tokens // GROUPS
    width = model // 4
    hid_rows = r.w_gate.shape[0]
    devices = CORES * GROUPS
    f32, b16 = jnp.float32, jnp.bfloat16
    far = [z, z + 1 - 2 * lax.rem(z, 2), z + 2 - 4 * lax.div(z, 2), 3 - z]
    peer = [(CORES * far[d] + c, t) for d in range(GROUPS)]
    mate = (CORES * z + 1 - c, t)
    after, before = (lax.rem(s + 1, devices), t), (lax.rem(s + devices - 1, devices), t)
    side_z = lax.rem(z + GROUPS + 2 * c - 1, GROUPS)
    side = (CORES * side_z + 1 - c, t)
    lane = [(s, lanes[j]) for j in range(3)]
    mine = span(t, width)
    sub = width // 4
    mine_sub = span(t, sub)

    loads = {}
    order = ("moe", "cot", "gate_c", "value_x", "w_gate", "w_up", "w_down", "gate_b", "taps", "out_proj")
    for i, key in enumerate(order):
        loads[key] = pltpu.make_async_copy(getattr(r, key), getattr(r, "v_" + key), r.load.at[i])
        loads[key].start()
    targets = peer[1:] + [mate] + lane + [side]
    barrier = pltpu.get_barrier_semaphore()
    for target in targets:
        pl.semaphore_signal(barrier, inc=1, device_id=target, device_id_type=MESH)

    down = lax.broadcasted_iota(jnp.int32, (tokens, tokens), 0)
    along = lax.broadcasted_iota(jnp.int32, (tokens, tokens), 1)
    eye = down == along

    def column(row):
        return jnp.sum(jnp.where(eye, row, 0.0), axis=1, keepdims=True)

    lead = r.routing[0:1, :]
    group = lax.div(lead, CORES)
    low, high = lax.rem(group, 2), lax.div(group, 2)
    z_low, z_high = lax.rem(z, 2), lax.div(z, 2)
    slot = (low + z_low - 2 * low * z_low) + 2 * (high + z_high - 2 * high * z_high)
    slot = slot.astype(f32)
    earlier = (column(slot) == slot) & (down < along)
    rank = jnp.sum(jnp.where(earlier, 1.0, 0.0), axis=0, keepdims=True)
    at_row = slot * cap + rank
    at_col = column(at_row)
    select = (at_row == down.astype(f32)).astype(f32).astype(b16)
    r.pick[...] = select
    unselect = (at_col == along.astype(f32)).astype(f32).astype(b16)
    for a, key in enumerate(("moe", "cot")):
        loads[key].wait()
        for n in range(4):
            cols = slice(n * width, (n + 1) * width)
            r.rows[a, :, :, cols] = (
                plain(select, getattr(r, "v_" + key)[:, cols]).astype(b16).reshape(GROUPS, cap, width)
            )
    for a in range(2):
        r.land[a, 0, c] = r.rows[a, 0]
    pl.semaphore_wait(barrier, len(targets))

    steps = [(a, d) for d in range(1, GROUPS) for a in range(2)]
    copies = []

    def send(*args):
        copy = remote(*args)
        copy.start()
        copies.append(copy)
        return copy

    first, small = {}, {}
    for a, d in steps[:2]:
        first[a, d] = send(
            r.rows.at[a, d, :, mine],
            r.land.at[a, d, c, :, mine],
            r.sz.at[a, d - 1],
            r.rz.at[a, d - 1],
            peer[d],
        )
    fourth, small_mate = {}, {}
    for a in range(2):
        fourth[a, 0] = send(
            r.rows.at[a, 0], r.land.at[a, 0, c], r.sm.at[a, 0], r.rm.at[a, 0], mate
        )
    is_even = lax.rem(lead, CORES) == 0
    by_core = [
        column(jnp.where(is_even, r.route_weight[k : k + 1, :], r.route_weight[1 - k : 2 - k, :]))
        for k in range(CORES)
    ]
    lane_at = lax.broadcasted_iota(jnp.int32, (tokens, 128), 1).astype(f32)
    row_at = lax.broadcasted_iota(jnp.int32, (8, 128), 0)
    for d in range(GROUPS):
        hit = at_col == lane_at + float(d * cap)
        picked = [jnp.sum(jnp.where(hit, by_core[k], 0.0), axis=0, keepdims=True) for k in range(CORES)]
        r.weights[d] = jnp.where(row_at == 0, picked[0], picked[1])
    r.weight_in[0, c] = r.weights[0]
    for d in range(1, GROUPS):
        small[d] = send(r.weights.at[d], r.weight_in.at[d, c], r.sw.at[d - 1], r.rw.at[d - 1], peer[d])
    small_mate[0] = send(
        r.weights.at[0], r.weight_in.at[0, c], r.sv.at[0], r.rv.at[0], mate
    )
    loads["gate_c"].wait()
    loads["value_x"].wait()
    mixed = (r.v_gate_c[...].astype(f32) * r.v_value_x[...].astype(f32)).astype(b16).astype(f32)
    r.edge[...] = mixed[tokens - 8 :, :]
    halo = send(r.edge, r.edge_in, r.sh.at[0], r.rh.at[0], after)

    for a, d in steps[2:]:
        first[a, d] = send(
            r.rows.at[a, d, :, mine],
            r.land.at[a, d, c, :, mine],
            r.sz.at[a, d - 1],
            r.rz.at[a, d - 1],
            peer[d],
        )

    second, third = {}, {}

    def e1(a, d):
        first[a, d].wait_recv()
        block = r.land.at[a, d, c, :, mine]
        for j in range(2):
            second[a, d, j] = send(block, block, r.sx.at[a, d - 1, j], r.rx.at[a, d - 1, j], lane[j])
        if a == 1:
            small[d].wait_recv()
            block = r.weight_in.at[d, c]
            small_mate[d] = send(block, block, r.sv.at[d], r.rv.at[d], mate)

    def e2(a, d):
        for j in range(2):
            second[a, d, j].wait_recv()
        for j in range(2):
            block = r.land.at[a, d, c, :, half(lanes[1 - j], j, width)]
            third[a, d, j] = send(block, block, r.sy.at[a, d - 1, j], r.ry.at[a, d - 1, j], lane[j])

    def e3(a, d):
        for j in range(2):
            third[a, d, j].wait_recv()
        block = r.land.at[a, d, c]
        fourth[a, d] = send(block, block, r.sm.at[a, d], r.rm.at[a, d], mate)

    def e4(a, d):
        fourth[a, d].wait_recv()

    cap_down = lax.broadcasted_iota(jnp.int32, (cap, 128), 0)
    cap_along = lax.broadcasted_iota(jnp.int32, (cap, 128), 1)

    unit = lax.broadcasted_iota(jnp.int32, (256, 256), 0) == lax.broadcasted_iota(
        jnp.int32, (256, 256), 1
    )
    r.unit[...] = unit.astype(f32).astype(b16)
    turns = ("w_gate", "w_up", "w_down")

    def turn(i, first_tile, count):
        source, out = getattr(r, "v_" + turns[i]), r.turned
        for n in range(first_tile, first_tile + count):
            at = slice(n * 256, (n + 1) * 256)
            out[i, at, :] = last_dims(r.unit[...], source[:, at]).astype(b16)

    def forward(d):
        small_mate[d].wait_recv()
        for k in range(CORES):
            tile = r.weight_in[d, k]
            row = jnp.sum(jnp.where(row_at == c, tile, 0.0), axis=0, keepdims=True)
            scale = jnp.sum(jnp.where(cap_down == cap_along, row, 0.0), axis=1, keepdims=True)
            r.scaled[d, k] = (scale * r.land[1, d, k].astype(f32)).astype(b16)
        x = r.land[0, d].reshape(CORES * cap, model)
        y = r.scaled[d].reshape(CORES * cap, model)
        block = hid_rows // 2
        for n in range(2):
            hs = slice(n * block, (n + 1) * block)
            if d == 0:
                gate = last_dims(x, r.v_w_gate[hs, :])
                up = last_dims(x, r.v_w_up[hs, :])
                grad = last_dims(y, r.v_w_down[hs, :])
            else:
                gate = plain(x, r.turned[0, :, hs])
                up = plain(x, r.turned[1, :, hs])
                grad = plain(y, r.turned[2, :, hs])
            sig = jax.nn.sigmoid(gate)
            silu = gate * sig
            r.hidden[d, :, hs] = (silu * up).astype(b16)
            r.gate_grad[d, :, hs] = (grad * up * sig * (1.0 + gate * (1.0 - sig))).astype(b16)
            r.up_grad[d, :, hs] = (grad * silu).astype(b16)

    swap, across, hop, home, spread, relay = {}, {}, {}, {}, {}, {}
    piece, fan, pass_on = {}, {}, {}

    def backward(d):
        for n in range(4):
            cols = slice(n * width, (n + 1) * width)
            value = plain(r.gate_grad[d], r.v_w_gate[:, cols]) + plain(
                r.up_grad[d], r.v_w_up[:, cols]
            )
            value = value.astype(b16).reshape(CORES, cap, width)
            for q in range(4):
                at = q * width + n * sub
                r.part[d, :, :, at : at + sub] = value[:, :, q * sub : (q + 1) * sub]
        swap[d] = send(r.part.at[d, 1 - c], r.mate_in.at[d], r.sa.at[d], r.ra.at[d], mate)

    def reduce_start(d):
        swap[d].wait_recv()
        r.total[d] = (r.part[d, c].astype(f32) + r.mate_in[d].astype(f32)).astype(b16)
        for j in range(2):
            for i, target in enumerate((2, j)):
                across[d, j, 1 - i] = send(
                    r.total.at[d, :, half(lanes[target], j, width)],
                    r.lane_in.at[d, j, 1 - i],
                    r.sb.at[d, j, 1 - i],
                    r.rb.at[d, j, 1 - i],
                    lane[j],
                )

    def reduce_mid(d):
        for j in range(2):
            across[d, j, 1].wait_recv()
            value = r.total[d, :, half(lanes[1 - j], j, width)].astype(f32) + r.lane_in[d, j, 1].astype(f32)
            r.hop[d, j] = value.astype(b16)
            hop[d, j] = send(r.hop.at[d, j], r.hop_in.at[d, j], r.sg.at[d, j], r.rg.at[d, j], lane[1 - j])

    def spread_start(d):
        block = r.home.at[d, :, mine]
        for j in range(2):
            spread[d, j] = send(block, block, r.sd.at[d, j], r.rd.at[d, j], lane[j])

    def reduce_end(d):
        for j in range(2):
            across[d, j, 0].wait_recv()
            hop[d, j].wait_recv()
            value = r.total[d, :, half(t, j, width)].astype(f32) + r.lane_in[d, j, 0].astype(f32)
            value = value + r.hop_in[d, j].astype(f32)
            r.done[d, :, j * (width // 2) : (j + 1) * (width // 2)] = value.astype(b16)
        if d > 0:
            home[d] = send(
                r.done.at[d], r.home.at[d, :, mine], r.sc.at[d - 1], r.rc.at[d - 1], peer[d]
            )
        for e in (3, 2, 1, 0):
            own = pl.ds(pl.multiple_of(far[e] * width + t * sub, sub), sub)
            value = r.land[1, d, c, :, own].astype(f32) + r.done[d, :, span(far[e], sub)].astype(f32)
            if e > 0:
                r.op_out[d, e - 1] = value.astype(b16)
                piece[d, e] = send(
                    r.op_out.at[d, e - 1],
                    r.op.at[e, d, :, mine_sub],
                    r.sp.at[d, e - 1],
                    r.rp.at[d, e - 1],
                    peer[e],
                )
            else:
                r.op[0, d, :, mine_sub] = value.astype(b16)
        if d == 0:
            r.home[0, :, mine] = r.done[0]
            spread_start(0)

    def fan_start(d):
        for e in range(1, GROUPS):
            piece[d, e].wait_recv()
        block = r.op.at[:, d, :, mine_sub]
        for j in range(2):
            fan[d, j] = send(block, block, r.sq.at[d, j], r.rq.at[d, j], lane[j])

    def pass_start(d):
        for j in range(2):
            fan[d, j].wait_recv()
        for j in range(2):
            block = r.op.at[2 * j : 2 * j + 2, d, :, span(lanes[1 - j], sub)]
            pass_on[d, j] = send(block, block, r.so.at[d, j], r.ro.at[d, j], lane[j])

    def pass_end(d):
        for j in range(2):
            pass_on[d, j].wait_recv()

    def home_in(d):
        home[d].wait_recv()
        spread_start(d)

    def relay_start(d):
        for j in range(2):
            spread[d, j].wait_recv()
        for j in range(2):
            block = r.home.at[d, :, half(lanes[1 - j], j, width)]
            relay[d, j] = send(block, block, r.se.at[d, j], r.re.at[d, j], lane[j])

    def relay_end(d):
        for j in range(2):
            relay[d, j].wait_recv()

    sources = (("w_gate_grad", "gate_grad", 0), ("w_up_grad", "up_grad", 0), ("w_down_grad", "hidden", 1))

    def weight_grad(i, *tiles):
        out, left, a = sources[i]
        lhs = getattr(r, left)[...].reshape(GROUPS * CORES * cap, hid_rows)
        for n in tiles:
            cols = slice(n * width, (n + 1) * width)
            rhs = r.land[0, :, :, :, cols] if a == 0 else r.scaled[:, :, :, cols]
            getattr(r, out)[:, cols] = first_dims(lhs, rhs.reshape(GROUPS * CORES * cap, width)).astype(b16)

    token_at = lax.broadcasted_iota(jnp.int32, (tokens, chan), 0)

    def conv_forward():
        halo.wait_recv()
        loads["taps"].wait()
        loads["gate_b"].wait()
        keep = jnp.where(s == 0, 0.0, 1.0)
        one, two = keep * r.edge_in[7:8, :], keep * r.edge_in[6:7, :]
        back_one = jnp.where(token_at == 0, one, pltpu.roll(mixed, 1, 0))
        back_two = jnp.where(
            token_at == 0, two, jnp.where(token_at == 1, one, pltpu.roll(mixed, 2, 0))
        )
        taps = r.v_taps
        conv = taps[0:1, :] * back_two + taps[1:2, :] * back_one + taps[2:3, :] * mixed
        r.conv[...] = conv
        act = (r.v_gate_b[...].astype(f32) * conv).astype(b16)
        r.act_in[0] = plain(r.pick[...], act).astype(b16).reshape(GROUPS, cap, chan)

    action = {}

    def act_start():
        for d in (3, 2, 1):
            action[d] = send(
                r.act_in.at[0], r.act_in.at[d], r.su.at[d - 1], r.ru.at[d - 1], peer[d]
            )

    def stream_of(pull, n):
        slabs = [r.home[:, :, q * width + n * sub : q * width + (n + 1) * sub] for q in range(4)]
        slab = jnp.concatenate(slabs, axis=2).reshape(tokens, width)
        return plain(pull, slab).astype(b16)

    last = {}

    def rim_start():
        for d in range(GROUPS):
            relay_end(d)
        loads["out_proj"].wait()
        for n in range(4):
            cols = slice(n * width, (n + 1) * width)
            full = stream_of(unselect[0:16, :], n)
            r.stream[0:16, cols] = (r.v_cot[0:16, cols].astype(f32) + full.astype(f32)).astype(b16)
        top = last_dims(r.stream[0:16, :], r.v_out_proj[...])[0:8, :]
        r.rim[...] = top * r.v_gate_b[0:16, :].astype(f32)[0:8, :]
        last[0] = send(r.rim, r.rim_in, r.sh.at[1], r.rh.at[1], before)

    def project():
        for d in range(1, GROUPS):
            action[d].wait_recv()
        for e in range(GROUPS):
            for d in range(GROUPS):
                r.mix[e, d] = r.act_in[e ^ d, d]
        for d in range(GROUPS):
            pass_end(d)
        narrow = width // CORES
        rows_all = GROUPS * GROUPS * cap
        mix = r.mix[...].reshape(rows_all, chan)
        there = r.op[:, :, :, span(1 - c, narrow)].reshape(rows_all, narrow)
        r.give[...] = first_dims(mix, there).astype(b16)
        last[1] = send(r.give, r.take, r.sn.at[0], r.rn.at[0], mate)
        here = r.op[:, :, :, span(c, narrow)].reshape(rows_all, narrow)
        r.proj_grad[...] = first_dims(mix, here)

    def stream_all():
        for n in range(4):
            cols = slice(n * width, (n + 1) * width)
            full = stream_of(unselect, n)
            r.full[:, cols] = full
            r.stream[:, cols] = (r.v_cot[:, cols].astype(f32) + full.astype(f32)).astype(b16)

    loads["w_gate"].wait()
    loads["w_up"].wait()
    loads["w_down"].wait()
    turn(1, 6, 2)
    e4(0, 0)
    e4(1, 0)
    forward(0)
    e1(*steps[0])
    e1(*steps[1])
    turn(1, 2, 2)
    e1(*steps[2])
    backward(0)
    e1(*steps[3])
    turn(1, 4, 2)
    turn(0, 0, 2)
    conv_forward()
    e2(*steps[0])
    turn(2, 2, 2)
    e2(*steps[1])
    turn(2, 6, 2)
    e1(*steps[4])
    turn(0, 2, 2)
    e2(*steps[2])
    e2(*steps[3])
    e1(*steps[5])
    turn(0, 6, 2)
    turn(0, 4, 2)
    act_start()
    turn(1, 0, 2)
    turn(2, 4, 2)
    e3(*steps[1])
    e3(*steps[0])
    reduce_start(0)
    e3(*steps[2])
    e2(*steps[4])
    turn(2, 0, 2)
    e3(*steps[3])
    e4(0, 1)
    e4(1, 1)
    forward(1)
    e2(*steps[5])
    backward(1)
    reduce_mid(0)
    e4(0, 2)
    e4(1, 2)
    forward(2)
    e3(*steps[4])
    backward(2)
    reduce_start(1)
    e3(*steps[5])
    reduce_start(2)
    reduce_end(0)
    e4(0, 3)
    e4(1, 3)
    forward(3)
    backward(3)
    reduce_mid(1)
    weight_grad(0, 2)
    reduce_mid(2)
    reduce_start(3)
    reduce_end(1)
    fan_start(0)
    reduce_end(2)
    reduce_mid(3)
    relay_start(0)
    home_in(1)
    fan_start(1)
    reduce_end(3)
    weight_grad(2, 3)
    weight_grad(2, 0)
    pass_start(0)
    weight_grad(1, 0)
    home_in(2)
    relay_start(1)
    weight_grad(1, 2)
    weight_grad(0, 1)
    pass_start(1)
    fan_start(2)
    weight_grad(0, 3)
    home_in(3)
    fan_start(3)
    weight_grad(1, 1)
    relay_start(2)
    weight_grad(0, 0)
    weight_grad(1, 3)
    weight_grad(2, 2)
    pass_start(2)
    relay_start(3)
    weight_grad(2, 1)
    pass_start(3)
    rim_start()
    project()
    stream_all()
    act_grad = last_dims(r.stream[...], r.v_out_proj[...])
    conv_grad = act_grad * r.v_gate_b[...].astype(f32)
    r.moe_in_grad[...] = r.full[:, mine]
    r.gate_b_grad[...] = (act_grad * r.conv[...]).astype(b16)
    last[0].wait_recv()
    keep = jnp.where(s == devices - 1, 0.0, 1.0)
    one, two = keep * r.rim_in[0:1, :], keep * r.rim_in[1:2, :]
    next_one = jnp.where(token_at == tokens - 1, one, pltpu.roll(conv_grad, tokens - 1, 0))
    next_two = jnp.where(
        token_at == tokens - 1,
        two,
        jnp.where(token_at == tokens - 2, one, pltpu.roll(conv_grad, tokens - 2, 0)),
    )
    taps = r.v_taps
    mixed_grad = taps[0:1, :] * next_two + taps[1:2, :] * next_one + taps[2:3, :] * conv_grad
    r.gate_c_grad[...] = (mixed_grad * r.v_value_x[...].astype(f32)).astype(b16)
    r.value_x_grad[...] = (mixed_grad * r.v_gate_c[...].astype(f32)).astype(b16)
    last[1].wait_recv()
    r.proj_grad[...] = r.proj_grad[...] + r.take[...].astype(f32)
    for copy in copies:
        copy.wait_send()


def store_kernel(*refs):
    count = len(refs) // 2
    copies = [pltpu.make_async_copy(refs[i], refs[count + i], refs[-1].at[i]) for i in range(count)]
    for copy in copies:
        copy.start()
    for copy in copies:
        copy.wait()


def on_device_paired(
    moe_in, cotangent, routing, route_weight, w_gate, w_up, w_down, gate_b, gate_c, value_x, conv_taps, out_proj
):
    tokens, model = moe_in.shape
    hid_rows = w_gate.shape[1]
    chan = gate_b.shape[0]
    cap, width = tokens // GROUPS, model // 4
    b16, f32 = moe_in.dtype, jnp.float32
    vmem, hbm = pl.BlockSpec(memory_space=pltpu.VMEM), pl.BlockSpec(memory_space=pltpu.HBM)
    dma = pltpu.SemaphoreType.DMA
    inputs = dict(
        routing=routing.T,
        route_weight=route_weight.T,
        moe=moe_in,
        cot=cotangent,
        w_gate=w_gate[0],
        w_up=w_up[0],
        w_down=w_down[0],
        gate_b=gate_b.T,
        gate_c=gate_c.T,
        value_x=value_x.T,
        taps=conv_taps,
        out_proj=out_proj,
    )
    outputs = dict(
        w_gate_grad=((hid_rows, model), b16),
        w_up_grad=((hid_rows, model), b16),
        w_down_grad=((hid_rows, model), b16),
        moe_in_grad=((tokens, width), b16),
        proj_grad=((chan, width // CORES), f32),
        gate_b_grad=((tokens, chan), b16),
        gate_c_grad=((tokens, chan), b16),
        value_x_grad=((tokens, chan), b16),
    )
    loaded = [key for key in inputs if key not in ("routing", "route_weight")]
    scratch = {"v_" + key: pltpu.VMEM(inputs[key].shape, inputs[key].dtype) for key in loaded}
    three, pair = GROUPS - 1, CORES * cap
    scratch |= dict(
        weights=pltpu.VMEM((GROUPS, 8, 128), f32),
        weight_in=pltpu.VMEM((GROUPS, CORES, 8, 128), f32),
        rows=pltpu.VMEM((2, GROUPS, cap, model), b16),
        land=pltpu.VMEM((2, GROUPS, CORES, cap, model), b16),
        scaled=pltpu.VMEM((GROUPS, CORES, cap, model), b16),
        hidden=pltpu.VMEM((GROUPS, pair, hid_rows), b16),
        gate_grad=pltpu.VMEM((GROUPS, pair, hid_rows), b16),
        up_grad=pltpu.VMEM((GROUPS, pair, hid_rows), b16),
        part=pltpu.VMEM((GROUPS, CORES, cap, model), b16),
        mate_in=pltpu.VMEM((GROUPS, cap, model), b16),
        total=pltpu.VMEM((GROUPS, cap, model), b16),
        lane_in=pltpu.VMEM((GROUPS, 2, 2, cap, width // 2), b16),
        done=pltpu.VMEM((GROUPS, cap, width), b16),
        home=pltpu.VMEM((GROUPS, cap, model), b16),
        full=pltpu.VMEM((tokens, model), b16),
        stream=pltpu.VMEM((tokens, model), b16),
        conv=pltpu.VMEM((tokens, chan), f32),
        edge=pltpu.VMEM((8, chan), f32),
        edge_in=pltpu.VMEM((8, chan), f32),
        rim=pltpu.VMEM((8, chan), f32),
        rim_in=pltpu.VMEM((8, chan), f32),
        give=pltpu.VMEM((chan, width // CORES), b16),
        take=pltpu.VMEM((chan, width // CORES), b16),
        unit=pltpu.VMEM((256, 256), b16),
        turned=pltpu.VMEM((3, model, hid_rows), b16),
        pick=pltpu.VMEM((tokens, tokens), b16),
        hop=pltpu.VMEM((GROUPS, 2, cap, width // 2), b16),
        hop_in=pltpu.VMEM((GROUPS, 2, cap, width // 2), b16),
        op=pltpu.VMEM((GROUPS, GROUPS, cap, width), b16),
        op_out=pltpu.VMEM((GROUPS, three, cap, width // 4), b16),
        act_in=pltpu.VMEM((GROUPS, GROUPS, cap, chan), b16),
        mix=pltpu.VMEM((GROUPS, GROUPS, cap, chan), b16),
        load=dma((len(loaded),)),
    )
    counts = dict(
        z=(2, three),
        w=(three,),
        x=(2, three, 2),
        y=(2, three, 2),
        m=(2, GROUPS),
        v=(GROUPS,),
        h=(2,),
        a=(GROUPS,),
        b=(GROUPS, 2, 2),
        g=(GROUPS, 2),
        c=(three,),
        d=(GROUPS, 2),
        e=(GROUPS, 2),
        p=(GROUPS, three),
        q=(GROUPS, 2),
        o=(GROUPS, 2),
        u=(three,),
        n=(1,),
    )
    for key, shape in counts.items():
        scratch["s" + key] = dma(shape)
        scratch["r" + key] = dma(shape)
    names = list(inputs) + list(outputs) + list(scratch)
    out = pl.pallas_call(
        functools.partial(step_kernel, names),
        out_shape=tuple(pltpu.VMEM(*shape) for shape in outputs.values()),
        in_specs=[hbm if key in loaded else vmem for key in inputs],
        out_specs=(vmem,) * len(outputs),
        scratch_shapes=list(scratch.values()),
        compiler_params=pltpu.CompilerParams(
            collective_id=0, has_side_effects=True, vmem_limit_bytes=54 * 1024 * 1024
        ),
        name="step",
    )(*inputs.values())
    out = pl.pallas_call(
        store_kernel,
        out_shape=tuple(jax.ShapeDtypeStruct(*shape) for shape in outputs.values()),
        in_specs=[vmem] * len(outputs),
        out_specs=(hbm,) * len(outputs),
        scratch_shapes=[dma((len(outputs),))],
        compiler_params=pltpu.CompilerParams(vmem_limit_bytes=4 * 1024 * 1024),
        name="store",
    )(*out)
    out = types.SimpleNamespace(**dict(zip(outputs, out)))
    return (
        out.w_gate_grad[None],
        out.w_up_grad[None],
        out.w_down_grad[None],
        out.moe_in_grad,
        out.proj_grad,
        out.gate_b_grad.T,
        out.gate_c_grad.T,
        out.value_x_grad.T,
    )


def on_device(*args):
    routes = args[2].shape[1]
    experts, lane_count = lax.axis_size("sp"), lax.axis_size("tp")
    if experts == CORES * GROUPS and routes == CORES and lane_count == 4:
        return on_device_paired(*args)
    return on_device_general(*args)


def solution(mesh):
    in_specs = (
        P("sp", None),
        P("sp", None),
        P("sp", None),
        P("sp", None),
        P("sp", "tp", None),
        P("sp", "tp", None),
        P("sp", "tp", None),
        P("tp", "sp"),
        P("tp", "sp"),
        P("tp", "sp"),
        P(None, "tp"),
        P("tp", None),
    )
    out_specs = (
        P("sp", "tp", None),
        P("sp", "tp", None),
        P("sp", "tp", None),
        P("sp", "tp"),
        P("tp", "sp"),
        P("tp", "sp"),
        P("tp", "sp"),
        P("tp", "sp"),
    )
    return jax.shard_map(
        on_device, mesh=mesh, in_specs=in_specs, out_specs=out_specs, check_vma=False
    )
```

```python
import functools
import types

import jax
import jax.numpy as jnp
from jax import lax
from jax.experimental import pallas as pl
from jax.experimental.pallas import tpu as pltpu
from jax.sharding import PartitionSpec as P

TAPS = 3
GROUPS = 4
CORES = 2
MESH = pl.DeviceIdType.MESH


def place():
    s, t = lax.axis_index("sp"), lax.axis_index("tp")
    z, c = lax.div(s, CORES), lax.rem(s, CORES)
    x, y = lax.rem(t, 2), lax.div(t, 2)
    lanes = (t + 1 - 2 * x, t + 2 - 4 * y, 3 - t)
    return s, t, z, c, lanes


def span(index, width):
    return pl.ds(pl.multiple_of(index * width, width), width)


def remote(src, dst, send_sem, recv_sem, target):
    return pltpu.make_async_remote_copy(
        src_ref=src,
        dst_ref=dst,
        send_sem=send_sem,
        recv_sem=recv_sem,
        device_id=target,
        device_id_type=MESH,
    )


def half(quarter, side, width):
    return pl.ds(pl.multiple_of(quarter * width + side * (width // 2), width // 2), width // 2)


def from_behind(array, axis, by):
    count = lax.axis_size(axis)
    pairs = [(i, i + by) for i in range(count) if 0 <= i + by < count]
    return lax.ppermute(array, axis, pairs)


def on_device_general(
    moe_in,
    cotangent,
    routing,
    route_weight,
    w_gate,
    w_up,
    w_down,
    gate_b,
    gate_c,
    value_x,
    conv_taps,
    out_proj,
):
    tok_rows = routing.shape[0]
    top_routes = routing.shape[1]
    experts = lax.axis_size("sp")
    lane_count = lax.axis_size("tp")
    model_width = moe_in.shape[1]
    capacity = top_routes * tok_rows // experts
    flat_routes = routing.reshape(-1)
    route_count = flat_routes.shape[0]
    one_hot = (flat_routes[:, None] == jnp.arange(experts, dtype=jnp.int32)[None, :]).astype(
        jnp.int32
    )
    slot_rank = jnp.sum(jnp.cumsum(one_hot, axis=0) * one_hot, axis=1) - 1
    slot_index = flat_routes * capacity + slot_rank
    source = (
        jnp.zeros((route_count,), jnp.int32)
        .at[slot_index]
        .set(jnp.arange(route_count, dtype=jnp.int32))
    )
    owner_token = source // top_routes
    scales = route_weight.reshape(-1)[source][:, None]
    col_width = model_width // lane_count
    col_start = lax.axis_index("tp") * col_width
    rows_part = lax.dynamic_slice_in_dim(moe_in, col_start, col_width, 1)[owner_token]
    cot_slice = lax.dynamic_slice_in_dim(cotangent, col_start, col_width, 1)[owner_token]
    cot_part = (scales * cot_slice.astype(jnp.float32)).astype(jnp.bfloat16)
    moved = (
        lax.all_to_all(rows_part, "sp", split_axis=0, concat_axis=0, tiled=True),
        lax.all_to_all(cot_part, "sp", split_axis=0, concat_axis=0, tiled=True),
    )
    arrived, arrived_cot = (
        lax.all_gather(moved[0], "tp", axis=1, tiled=True),
        lax.all_gather(moved[1], "tp", axis=1, tiled=True),
    )
    contract_model = (((1,), (1,)), ((), ()))
    over_rows = (((0,), (0,)), ((), ()))
    gate_pre = lax.dot_general(
        arrived, w_gate[0], contract_model, preferred_element_type=jnp.float32
    )
    up_pre = lax.dot_general(arrived, w_up[0], contract_model, preferred_element_type=jnp.float32)
    sigmoid_gate = jax.nn.sigmoid(gate_pre)
    hidden = (gate_pre * sigmoid_gate * up_pre).astype(jnp.bfloat16)
    hidden_grad = lax.dot_general(
        arrived_cot, w_down[0], contract_model, preferred_element_type=jnp.float32
    )
    gate_grad = (
        hidden_grad * up_pre * sigmoid_gate * (1.0 + gate_pre * (1.0 - sigmoid_gate))
    ).astype(jnp.bfloat16)
    up_grad = (hidden_grad * gate_pre * sigmoid_gate).astype(jnp.bfloat16)
    w_gate_grad = lax.dot_general(
        gate_grad, arrived, over_rows, preferred_element_type=jnp.float32
    ).astype(jnp.bfloat16)[None]
    w_up_grad = lax.dot_general(
        up_grad, arrived, over_rows, preferred_element_type=jnp.float32
    ).astype(jnp.bfloat16)[None]
    w_down_grad = lax.dot_general(
        hidden, arrived_cot, over_rows, preferred_element_type=jnp.float32
    ).astype(jnp.bfloat16)[None]
    partial_value = jnp.dot(gate_grad, w_gate[0], preferred_element_type=jnp.float32) + jnp.dot(
        up_grad, w_up[0], preferred_element_type=jnp.float32
    )
    partial_value = lax.optimization_barrier(partial_value.astype(jnp.bfloat16)).astype(jnp.float32)
    summed = lax.psum_scatter(
        partial_value.astype(jnp.bfloat16), "tp", scatter_dimension=1, tiled=True
    )
    returned = lax.all_to_all(summed, "sp", split_axis=0, concat_axis=0, tiled=True)
    per_route = returned[slot_index].astype(jnp.float32)
    moe_in_grad = jnp.sum(per_route.reshape(tok_rows, top_routes, -1), axis=1).astype(jnp.bfloat16)
    full_grad = lax.all_gather(moe_in_grad, "tp", axis=1, tiled=True)
    stream_grad = (cotangent.astype(jnp.float32) + full_grad.astype(jnp.float32)).astype(
        jnp.bfloat16
    )
    mixed_in = lax.optimization_barrier(
        (gate_c.astype(jnp.float32) * value_x.astype(jnp.float32)).astype(jnp.bfloat16)
    )
    earlier = from_behind(mixed_in[:, tok_rows - (TAPS - 1) :], "sp", 1)
    extended = jnp.concatenate([earlier, mixed_in], axis=1).astype(jnp.float32)
    conv_out = jnp.zeros(mixed_in.shape, jnp.float32)
    for tap in range(TAPS):
        conv_out = conv_out + conv_taps[tap][:, None] * extended[:, tap : tap + tok_rows]
    mixer_act = (gate_b.astype(jnp.float32) * conv_out).astype(jnp.bfloat16)
    act_grad = lax.dot_general(
        out_proj, stream_grad, contract_model, preferred_element_type=jnp.float32
    )
    proj_rows = lax.psum_scatter(
        lax.dot_general(
            stream_grad, mixer_act, (((0,), (1,)), ((), ())), preferred_element_type=jnp.float32
        ).astype(jnp.bfloat16),
        "sp",
        scatter_dimension=0,
        tiled=True,
    ).astype(jnp.float32)
    proj_grad = proj_rows.T
    gate_b_grad = (act_grad * conv_out).astype(jnp.bfloat16)
    conv_grad = act_grad * gate_b.astype(jnp.float32)
    later = from_behind(conv_grad[:, : TAPS - 1], "sp", -1)
    extended_grad = jnp.concatenate([conv_grad, later], axis=1)
    mixed_grad = jnp.zeros(conv_grad.shape, jnp.float32)
    for tap in range(TAPS):
        offset = TAPS - 1 - tap
        mixed_grad = (
            mixed_grad + conv_taps[tap][:, None] * extended_grad[:, offset : offset + tok_rows]
        )
    gate_c_grad = (mixed_grad * value_x.astype(jnp.float32)).astype(jnp.bfloat16)
    value_x_grad = (mixed_grad * gate_c.astype(jnp.float32)).astype(jnp.bfloat16)
    return (
        w_gate_grad,
        w_up_grad,
        w_down_grad,
        moe_in_grad,
        proj_grad,
        gate_b_grad,
        gate_c_grad,
        value_x_grad,
    )


def last_dims(lhs, rhs):
    return lax.dot_general(lhs, rhs, (((1,), (1,)), ((), ())), preferred_element_type=jnp.float32)


def first_dims(lhs, rhs):
    return lax.dot_general(lhs, rhs, (((0,), (0,)), ((), ())), preferred_element_type=jnp.float32)


def plain(lhs, rhs):
    return jnp.dot(lhs, rhs, preferred_element_type=jnp.float32)


def step_kernel(names, *refs):
    r = types.SimpleNamespace(**dict(zip(names, refs)))
    s, t, z, c, lanes = place()
    tokens, model = r.moe.shape
    chan = r.gate_b.shape[1]
    cap = tokens // GROUPS
    width = model // 4
    hid_rows = r.w_gate.shape[0]
    devices = CORES * GROUPS
    f32, b16 = jnp.float32, jnp.bfloat16
    far = [z, z + 1 - 2 * lax.rem(z, 2), z + 2 - 4 * lax.div(z, 2), 3 - z]
    peer = [(CORES * far[d] + c, t) for d in range(GROUPS)]
    mate = (CORES * z + 1 - c, t)
    after, before = (lax.rem(s + 1, devices), t), (lax.rem(s + devices - 1, devices), t)
    side_z = lax.rem(z + GROUPS + 2 * c - 1, GROUPS)
    side = (CORES * side_z + 1 - c, t)
    lane = [(s, lanes[j]) for j in range(3)]
    mine = span(t, width)
    sub = width // 4
    mine_sub = span(t, sub)

    loads = {}
    order = ("routing", "route_weight", "moe", "cot", "gate_c", "value_x", "w_gate", "w_up", "w_down", "gate_b", "taps", "out_proj")
    for i, key in enumerate(order):
        loads[key] = pltpu.make_async_copy(getattr(r, key), getattr(r, "v_" + key), r.load.at[i])
        loads[key].start()
    targets = peer[1:] + [mate] + lane + [side]
    barrier = pltpu.get_barrier_semaphore()
    for target in targets:
        pl.semaphore_signal(barrier, inc=1, device_id=target, device_id_type=MESH)

    down = lax.broadcasted_iota(jnp.int32, (tokens, tokens), 0)
    along = lax.broadcasted_iota(jnp.int32, (tokens, tokens), 1)
    eye = down == along

    def column(row):
        return jnp.sum(jnp.where(eye, row, 0.0), axis=1, keepdims=True)

    loads["routing"].wait()
    lead = r.v_routing[0:1, :]
    group = lax.div(lead, CORES)
    low, high = lax.rem(group, 2), lax.div(group, 2)
    z_low, z_high = lax.rem(z, 2), lax.div(z, 2)
    slot = (low + z_low - 2 * low * z_low) + 2 * (high + z_high - 2 * high * z_high)
    slot = slot.astype(f32)
    earlier = (column(slot) == slot) & (down < along)
    rank = jnp.sum(jnp.where(earlier, 1.0, 0.0), axis=0, keepdims=True)
    at_row = slot * cap + rank
    at_col = column(at_row)
    select = (at_row == down.astype(f32)).astype(f32).astype(b16)
    r.pick[...] = select
    unselect = (at_col == along.astype(f32)).astype(f32).astype(b16)
    for a, key in enumerate(("moe", "cot")):
        loads[key].wait()
        for n in range(4):
            cols = slice(n * width, (n + 1) * width)
            r.rows[a, :, :, cols] = (
                plain(select, getattr(r, "v_" + key)[:, cols]).astype(b16).reshape(GROUPS, cap, width)
            )
    for a in range(2):
        r.land[a, 0, c] = r.rows[a, 0]
    pl.semaphore_wait(barrier, len(targets))

    steps = [(a, d) for d in range(1, GROUPS) for a in range(2)]
    copies = []

    def send(*args):
        copy = remote(*args)
        copy.start()
        copies.append(copy)
        return copy

    first, small = {}, {}
    for a, d in steps[:2]:
        first[a, d] = send(
            r.rows.at[a, d, :, mine],
            r.land.at[a, d, c, :, mine],
            r.sz.at[a, d - 1],
            r.rz.at[a, d - 1],
            peer[d],
        )
    fourth, small_mate = {}, {}
    for a in range(2):
        fourth[a, 0] = send(
            r.rows.at[a, 0], r.land.at[a, 0, c], r.sm.at[a, 0], r.rm.at[a, 0], mate
        )
    loads["route_weight"].wait()
    is_even = lax.rem(lead, CORES) == 0
    by_core = [
        column(jnp.where(is_even, r.v_route_weight[k : k + 1, :], r.v_route_weight[1 - k : 2 - k, :]))
        for k in range(CORES)
    ]
    lane_at = lax.broadcasted_iota(jnp.int32, (tokens, 128), 1).astype(f32)
    row_at = lax.broadcasted_iota(jnp.int32, (8, 128), 0)
    for d in range(GROUPS):
        hit = at_col == lane_at + float(d * cap)
        picked = [jnp.sum(jnp.where(hit, by_core[k], 0.0), axis=0, keepdims=True) for k in range(CORES)]
        r.weights[d] = jnp.where(row_at == 0, picked[0], picked[1])
    r.weight_in[0, c] = r.weights[0]
    for d in range(1, GROUPS):
        small[d] = send(r.weights.at[d], r.weight_in.at[d, c], r.sw.at[d - 1], r.rw.at[d - 1], peer[d])
    small_mate[0] = send(
        r.weights.at[0], r.weight_in.at[0, c], r.sv.at[0], r.rv.at[0], mate
    )
    loads["gate_c"].wait()
    loads["value_x"].wait()
    mixed = (r.v_gate_c[...].astype(f32) * r.v_value_x[...].astype(f32)).astype(b16).astype(f32)
    r.edge[...] = mixed[tokens - 8 :, :]
    halo = send(r.edge, r.edge_in, r.sh.at[0], r.rh.at[0], after)

    for a, d in steps[2:]:
        first[a, d] = send(
            r.rows.at[a, d, :, mine],
            r.land.at[a, d, c, :, mine],
            r.sz.at[a, d - 1],
            r.rz.at[a, d - 1],
            peer[d],
        )

    second, third = {}, {}

    def e1(a, d):
        first[a, d].wait_recv()
        block = r.land.at[a, d, c, :, mine]
        for j in range(2):
            second[a, d, j] = send(block, block, r.sx.at[a, d - 1, j], r.rx.at[a, d - 1, j], lane[j])

    def e2(a, d):
        for j in range(2):
            second[a, d, j].wait_recv()
        for j in range(2):
            block = r.land.at[a, d, c, :, half(lanes[1 - j], j, width)]
            third[a, d, j] = send(block, block, r.sy.at[a, d - 1, j], r.ry.at[a, d - 1, j], lane[j])

    def e3(a, d):
        for j in range(2):
            third[a, d, j].wait_recv()
        block = r.land.at[a, d, c]
        fourth[a, d] = send(block, block, r.sm.at[a, d], r.rm.at[a, d], mate)
        if a == 1:
            small[d].wait_recv()
            block = r.weight_in.at[d, c]
            small_mate[d] = send(block, block, r.sv.at[d], r.rv.at[d], mate)

    def e4(a, d):
        fourth[a, d].wait_recv()

    cap_down = lax.broadcasted_iota(jnp.int32, (cap, 128), 0)
    cap_along = lax.broadcasted_iota(jnp.int32, (cap, 128), 1)

    unit = lax.broadcasted_iota(jnp.int32, (256, 256), 0) == lax.broadcasted_iota(
        jnp.int32, (256, 256), 1
    )
    r.unit[...] = unit.astype(f32).astype(b16)
    turns = ("w_gate", "w_up", "w_down")

    def turn(i, first_tile, count):
        source, out = getattr(r, "v_" + turns[i]), r.turned
        for n in range(first_tile, first_tile + count):
            at = slice(n * 256, (n + 1) * 256)
            out[i, at, :] = last_dims(r.unit[...], source[:, at]).astype(b16)

    def forward(d):
        small_mate[d].wait_recv()
        for k in range(CORES):
            tile = r.weight_in[d, k]
            row = jnp.sum(jnp.where(row_at == c, tile, 0.0), axis=0, keepdims=True)
            scale = jnp.sum(jnp.where(cap_down == cap_along, row, 0.0), axis=1, keepdims=True)
            r.scaled[d, k] = (scale * r.land[1, d, k].astype(f32)).astype(b16)
        x = r.land[0, d].reshape(CORES * cap, model)
        y = r.scaled[d].reshape(CORES * cap, model)
        block = hid_rows // 2
        for n in range(2):
            hs = slice(n * block, (n + 1) * block)
            if d == 0:
                gate = last_dims(x, r.v_w_gate[hs, :])
                up = last_dims(x, r.v_w_up[hs, :])
                grad = last_dims(y, r.v_w_down[hs, :])
            else:
                gate = plain(x, r.turned[0, :, hs])
                up = plain(x, r.turned[1, :, hs])
                grad = plain(y, r.turned[2, :, hs])
            sig = jax.nn.sigmoid(gate)
            silu = gate * sig
            r.hidden[d, :, hs] = (silu * up).astype(b16)
            r.gate_grad[d, :, hs] = (grad * up * sig * (1.0 + gate * (1.0 - sig))).astype(b16)
            r.up_grad[d, :, hs] = (grad * silu).astype(b16)

    swap, across, hop, home, spread, relay = {}, {}, {}, {}, {}, {}
    piece, fan, pass_on = {}, {}, {}

    def backward(d):
        for n in range(4):
            cols = slice(n * width, (n + 1) * width)
            value = plain(r.gate_grad[d], r.v_w_gate[:, cols]) + plain(
                r.up_grad[d], r.v_w_up[:, cols]
            )
            value = value.astype(b16).reshape(CORES, cap, width)
            for q in range(4):
                at = q * width + n * sub
                r.part[d, :, :, at : at + sub] = value[:, :, q * sub : (q + 1) * sub]
        swap[d] = send(r.part.at[d, 1 - c], r.mate_in.at[d], r.sa.at[d], r.ra.at[d], mate)

    def reduce_start(d):
        swap[d].wait_recv()
        r.total[d] = (r.part[d, c].astype(f32) + r.mate_in[d].astype(f32)).astype(b16)
        for j in range(2):
            for i, target in enumerate((2, j)):
                across[d, j, 1 - i] = send(
                    r.total.at[d, :, half(lanes[target], j, width)],
                    r.lane_in.at[d, j, 1 - i],
                    r.sb.at[d, j, 1 - i],
                    r.rb.at[d, j, 1 - i],
                    lane[j],
                )

    def reduce_mid(d):
        for j in range(2):
            across[d, j, 1].wait_recv()
            value = r.total[d, :, half(lanes[1 - j], j, width)].astype(f32) + r.lane_in[d, j, 1].astype(f32)
            r.hop[d, j] = value.astype(b16)
            hop[d, j] = send(r.hop.at[d, j], r.hop_in.at[d, j], r.sg.at[d, j], r.rg.at[d, j], lane[1 - j])

    def direct(d):
        return (2, 0, 1) if d >= 3 else (0, 1)

    def spread_start(d):
        block = r.home.at[d, :, mine]
        for j in direct(d):
            spread[d, j] = send(block, block, r.sd.at[d, j], r.rd.at[d, j], lane[j])

    def reduce_end(d):
        for j in range(2):
            across[d, j, 0].wait_recv()
            hop[d, j].wait_recv()
            value = r.total[d, :, half(t, j, width)].astype(f32) + r.lane_in[d, j, 0].astype(f32)
            value = value + r.hop_in[d, j].astype(f32)
            r.done[d, :, j * (width // 2) : (j + 1) * (width // 2)] = value.astype(b16)
        if d > 0:
            home[d] = send(
                r.done.at[d], r.home.at[d, :, mine], r.sc.at[d - 1], r.rc.at[d - 1], peer[d]
            )
        for e in (3, 2, 1, 0):
            own = pl.ds(pl.multiple_of(far[e] * width + t * sub, sub), sub)
            value = r.land[1, d, c, :, own].astype(f32) + r.done[d, :, span(far[e], sub)].astype(f32)
            if e > 0:
                r.op_out[d, e - 1] = value.astype(b16)
                piece[d, e] = send(
                    r.op_out.at[d, e - 1],
                    r.op.at[e, d, :, mine_sub],
                    r.sp.at[d, e - 1],
                    r.rp.at[d, e - 1],
                    peer[e],
                )
            else:
                r.op[0, d, :, mine_sub] = value.astype(b16)
        if d == 0:
            r.home[0, :, mine] = r.done[0]
            spread_start(0)

    def fan_start(d):
        for e in range(1, GROUPS):
            piece[d, e].wait_recv()
        block = r.op.at[:, d, :, mine_sub]
        for j in direct(d):
            fan[d, j] = send(block, block, r.sq.at[d, j], r.rq.at[d, j], lane[j])

    def pass_start(d):
        if len(direct(d)) == 3:
            return
        for j in range(2):
            fan[d, j].wait_recv()
        for j in range(2):
            block = r.op.at[2 * j : 2 * j + 2, d, :, span(lanes[1 - j], sub)]
            pass_on[d, j] = send(block, block, r.so.at[d, j], r.ro.at[d, j], lane[j])

    def pass_end(d):
        if len(direct(d)) == 3:
            for j in range(3):
                fan[d, j].wait_recv()
            return
        for j in range(2):
            pass_on[d, j].wait_recv()

    def home_in(d):
        home[d].wait_recv()
        spread_start(d)

    def relay_start(d):
        if len(direct(d)) == 3:
            return
        for j in range(2):
            spread[d, j].wait_recv()
        for j in range(2):
            block = r.home.at[d, :, half(lanes[1 - j], j, width)]
            relay[d, j] = send(block, block, r.se.at[d, j], r.re.at[d, j], lane[j])

    def relay_end(d):
        if len(direct(d)) == 3:
            for j in range(3):
                spread[d, j].wait_recv()
            return
        for j in range(2):
            relay[d, j].wait_recv()

    sources = (("w_gate_grad", "gate_grad", 0), ("w_up_grad", "up_grad", 0), ("w_down_grad", "hidden", 1))

    def weight_grad(i, *tiles):
        out, left, a = sources[i]
        lhs = getattr(r, left)[...].reshape(GROUPS * CORES * cap, hid_rows)
        for n in tiles:
            cols = slice(n * width, (n + 1) * width)
            rhs = r.land[0, :, :, :, cols] if a == 0 else r.scaled[:, :, :, cols]
            getattr(r, out)[:, cols] = first_dims(lhs, rhs.reshape(GROUPS * CORES * cap, width)).astype(b16)

    token_at = lax.broadcasted_iota(jnp.int32, (tokens, chan), 0)

    def conv_forward():
        halo.wait_recv()
        loads["taps"].wait()
        loads["gate_b"].wait()
        keep = jnp.where(s == 0, 0.0, 1.0)
        one, two = keep * r.edge_in[7:8, :], keep * r.edge_in[6:7, :]
        back_one = jnp.where(token_at == 0, one, pltpu.roll(mixed, 1, 0))
        back_two = jnp.where(
            token_at == 0, two, jnp.where(token_at == 1, one, pltpu.roll(mixed, 2, 0))
        )
        taps = r.v_taps
        conv = taps[0:1, :] * back_two + taps[1:2, :] * back_one + taps[2:3, :] * mixed
        r.conv[...] = conv
        act = (r.v_gate_b[...].astype(f32) * conv).astype(b16)
        r.act_in[0] = plain(r.pick[...], act).astype(b16).reshape(GROUPS, cap, chan)

    action = {}

    def act_start():
        for d in (3, 2, 1):
            action[d] = send(
                r.act_in.at[0], r.act_in.at[d], r.su.at[d - 1], r.ru.at[d - 1], peer[d]
            )

    def stream_of(pull, n):
        slabs = [r.home[:, :, q * width + n * sub : q * width + (n + 1) * sub] for q in range(4)]
        slab = jnp.concatenate(slabs, axis=2).reshape(tokens, width)
        return plain(pull, slab).astype(b16)

    last = {}

    def rim_start():
        for d in range(GROUPS):
            relay_end(d)
        loads["out_proj"].wait()
        for n in range(4):
            cols = slice(n * width, (n + 1) * width)
            full = stream_of(unselect[0:16, :], n)
            r.stream[0:16, cols] = (r.v_cot[0:16, cols].astype(f32) + full.astype(f32)).astype(b16)
        top = last_dims(r.stream[0:16, :], r.v_out_proj[...])[0:8, :]
        r.rim[...] = top * r.v_gate_b[0:16, :].astype(f32)[0:8, :]
        last[0] = send(r.rim, r.rim_in, r.sh.at[1], r.rh.at[1], before)

    def project():
        for d in range(1, GROUPS):
            action[d].wait_recv()
        for e in range(GROUPS):
            for d in range(GROUPS):
                r.mix[e, d] = r.act_in[e ^ d, d]
        for d in range(GROUPS):
            pass_end(d)
        narrow = width // CORES
        rows_all = GROUPS * GROUPS * cap
        mix = r.mix[...].reshape(rows_all, chan)
        there = r.op[:, :, :, span(1 - c, narrow)].reshape(rows_all, narrow)
        r.give[...] = first_dims(mix, there).astype(b16)
        last[1] = send(r.give, r.take, r.sn.at[0], r.rn.at[0], mate)
        here = r.op[:, :, :, span(c, narrow)].reshape(rows_all, narrow)
        r.proj_grad[...] = first_dims(mix, here)

    def stream_all():
        for n in range(4):
            cols = slice(n * width, (n + 1) * width)
            full = stream_of(unselect, n)
            r.full[:, cols] = full
            r.stream[:, cols] = (r.v_cot[:, cols].astype(f32) + full.astype(f32)).astype(b16)

    loads["w_gate"].wait()
    loads["w_up"].wait()
    loads["w_down"].wait()
    turn(2, 0, 2)
    e4(0, 0)
    e4(1, 0)
    forward(0)
    e1(*steps[0])
    conv_forward()
    e1(*steps[1])
    backward(0)
    turn(1, 2, 2)
    e1(*steps[2])
    turn(0, 4, 2)
    e1(*steps[3])
    turn(1, 0, 2)
    turn(0, 2, 2)
    e2(*steps[1])
    e2(*steps[0])
    turn(2, 4, 2)
    turn(1, 4, 2)
    e2(*steps[2])
    e1(*steps[5])
    act_start()
    turn(1, 6, 2)
    e2(*steps[3])
    e1(*steps[4])
    reduce_start(0)
    e3(*steps[1])
    turn(0, 6, 2)
    e3(*steps[0])
    turn(2, 2, 2)
    turn(0, 0, 2)
    e3(*steps[2])
    turn(2, 6, 2)
    e4(0, 1)
    e4(1, 1)
    forward(1)
    e3(*steps[3])
    e2(*steps[5])
    backward(1)
    e2(*steps[4])
    reduce_mid(0)
    e4(0, 2)
    e4(1, 2)
    forward(2)
    backward(2)
    e3(*steps[5])
    reduce_start(1)
    e3(*steps[4])
    reduce_start(2)
    reduce_end(0)
    e4(0, 3)
    e4(1, 3)
    forward(3)
    reduce_mid(1)
    backward(3)
    reduce_mid(2)
    weight_grad(0, 3)
    reduce_start(3)
    fan_start(0)
    relay_start(0)
    reduce_end(1)
    weight_grad(1, 0)
    weight_grad(0, 0)
    reduce_end(2)
    weight_grad(1, 1)
    reduce_mid(3)
    home_in(1)
    pass_start(0)
    weight_grad(2, 2)
    weight_grad(2, 1)
    fan_start(1)
    reduce_end(3)
    home_in(2)
    fan_start(2)
    pass_start(1)
    relay_start(1)
    relay_start(2)
    home_in(3)
    weight_grad(1, 2)
    weight_grad(2, 0)
    weight_grad(2, 3)
    fan_start(3)
    pass_start(2)
    weight_grad(0, 2)
    pass_start(3)
    weight_grad(1, 3)
    relay_start(3)
    weight_grad(0, 1)
    rim_start()
    stream_all()
    project()
    act_grad = last_dims(r.stream[...], r.v_out_proj[...])
    conv_grad = act_grad * r.v_gate_b[...].astype(f32)
    r.moe_in_grad[...] = r.full[:, mine]
    r.gate_b_grad[...] = (act_grad * r.conv[...]).astype(b16)
    last[0].wait_recv()
    keep = jnp.where(s == devices - 1, 0.0, 1.0)
    one, two = keep * r.rim_in[0:1, :], keep * r.rim_in[1:2, :]
    next_one = jnp.where(token_at == tokens - 1, one, pltpu.roll(conv_grad, tokens - 1, 0))
    next_two = jnp.where(
        token_at == tokens - 1,
        two,
        jnp.where(token_at == tokens - 2, one, pltpu.roll(conv_grad, tokens - 2, 0)),
    )
    taps = r.v_taps
    mixed_grad = taps[0:1, :] * next_two + taps[1:2, :] * next_one + taps[2:3, :] * conv_grad
    r.gate_c_grad[...] = (mixed_grad * r.v_value_x[...].astype(f32)).astype(b16)
    r.value_x_grad[...] = (mixed_grad * r.v_gate_c[...].astype(f32)).astype(b16)
    last[1].wait_recv()
    r.proj_grad[...] = r.proj_grad[...] + r.take[...].astype(f32)
    for copy in copies:
        copy.wait_send()


def store_kernel(*refs):
    count = len(refs) // 2
    copies = [pltpu.make_async_copy(refs[i], refs[count + i], refs[-1].at[i]) for i in range(count)]
    for copy in copies:
        copy.start()
    for copy in copies:
        copy.wait()


def on_device_paired(
    moe_in, cotangent, routing, route_weight, w_gate, w_up, w_down, gate_b, gate_c, value_x, conv_taps, out_proj
):
    tokens, model = moe_in.shape
    hid_rows = w_gate.shape[1]
    chan = gate_b.shape[0]
    cap, width = tokens // GROUPS, model // 4
    b16, f32 = moe_in.dtype, jnp.float32
    vmem, hbm = pl.BlockSpec(memory_space=pltpu.VMEM), pl.BlockSpec(memory_space=pltpu.HBM)
    dma = pltpu.SemaphoreType.DMA
    inputs = dict(
        routing=routing.T,
        route_weight=route_weight.T,
        moe=moe_in,
        cot=cotangent,
        w_gate=w_gate[0],
        w_up=w_up[0],
        w_down=w_down[0],
        gate_b=gate_b.T,
        gate_c=gate_c.T,
        value_x=value_x.T,
        taps=conv_taps,
        out_proj=out_proj,
    )
    outputs = dict(
        w_gate_grad=((hid_rows, model), b16),
        w_up_grad=((hid_rows, model), b16),
        w_down_grad=((hid_rows, model), b16),
        moe_in_grad=((tokens, width), b16),
        proj_grad=((chan, width // CORES), f32),
        gate_b_grad=((tokens, chan), b16),
        gate_c_grad=((tokens, chan), b16),
        value_x_grad=((tokens, chan), b16),
    )
    loaded = list(inputs)
    scratch = {"v_" + key: pltpu.VMEM(inputs[key].shape, inputs[key].dtype) for key in loaded}
    three, pair = GROUPS - 1, CORES * cap
    scratch |= dict(
        weights=pltpu.VMEM((GROUPS, 8, 128), f32),
        weight_in=pltpu.VMEM((GROUPS, CORES, 8, 128), f32),
        rows=pltpu.VMEM((2, GROUPS, cap, model), b16),
        land=pltpu.VMEM((2, GROUPS, CORES, cap, model), b16),
        scaled=pltpu.VMEM((GROUPS, CORES, cap, model), b16),
        hidden=pltpu.VMEM((GROUPS, pair, hid_rows), b16),
        gate_grad=pltpu.VMEM((GROUPS, pair, hid_rows), b16),
        up_grad=pltpu.VMEM((GROUPS, pair, hid_rows), b16),
        part=pltpu.VMEM((GROUPS, CORES, cap, model), b16),
        mate_in=pltpu.VMEM((GROUPS, cap, model), b16),
        total=pltpu.VMEM((GROUPS, cap, model), b16),
        lane_in=pltpu.VMEM((GROUPS, 2, 2, cap, width // 2), b16),
        done=pltpu.VMEM((GROUPS, cap, width), b16),
        home=pltpu.VMEM((GROUPS, cap, model), b16),
        full=pltpu.VMEM((tokens, model), b16),
        stream=pltpu.VMEM((tokens, model), b16),
        conv=pltpu.VMEM((tokens, chan), f32),
        edge=pltpu.VMEM((8, chan), f32),
        edge_in=pltpu.VMEM((8, chan), f32),
        rim=pltpu.VMEM((8, chan), f32),
        rim_in=pltpu.VMEM((8, chan), f32),
        give=pltpu.VMEM((chan, width // CORES), b16),
        take=pltpu.VMEM((chan, width // CORES), b16),
        unit=pltpu.VMEM((256, 256), b16),
        turned=pltpu.VMEM((3, model, hid_rows), b16),
        pick=pltpu.VMEM((tokens, tokens), b16),
        hop=pltpu.VMEM((GROUPS, 2, cap, width // 2), b16),
        hop_in=pltpu.VMEM((GROUPS, 2, cap, width // 2), b16),
        op=pltpu.VMEM((GROUPS, GROUPS, cap, width), b16),
        op_out=pltpu.VMEM((GROUPS, three, cap, width // 4), b16),
        act_in=pltpu.VMEM((GROUPS, GROUPS, cap, chan), b16),
        mix=pltpu.VMEM((GROUPS, GROUPS, cap, chan), b16),
        load=dma((len(loaded),)),
    )
    counts = dict(
        z=(2, three),
        w=(three,),
        x=(2, three, 2),
        y=(2, three, 2),
        m=(2, GROUPS),
        v=(GROUPS,),
        h=(2,),
        a=(GROUPS,),
        b=(GROUPS, 2, 2),
        g=(GROUPS, 2),
        c=(three,),
        d=(GROUPS, 3),
        e=(GROUPS, 2),
        p=(GROUPS, three),
        q=(GROUPS, 3),
        o=(GROUPS, 2),
        u=(three,),
        n=(1,),
    )
    for key, shape in counts.items():
        scratch["s" + key] = dma(shape)
        scratch["r" + key] = dma(shape)
    names = list(inputs) + list(outputs) + list(scratch)
    out = pl.pallas_call(
        functools.partial(step_kernel, names),
        out_shape=tuple(pltpu.VMEM(*shape) for shape in outputs.values()),
        in_specs=[hbm] * len(inputs),
        out_specs=(vmem,) * len(outputs),
        scratch_shapes=list(scratch.values()),
        compiler_params=pltpu.CompilerParams(
            collective_id=0, has_side_effects=True, vmem_limit_bytes=54 * 1024 * 1024
        ),
        name="step",
    )(*inputs.values())
    out = pl.pallas_call(
        store_kernel,
        out_shape=tuple(jax.ShapeDtypeStruct(*shape) for shape in outputs.values()),
        in_specs=[vmem] * len(outputs),
        out_specs=(hbm,) * len(outputs),
        scratch_shapes=[dma((len(outputs),))],
        compiler_params=pltpu.CompilerParams(vmem_limit_bytes=4 * 1024 * 1024),
        name="store",
    )(*out)
    out = types.SimpleNamespace(**dict(zip(outputs, out)))
    return (
        out.w_gate_grad[None],
        out.w_up_grad[None],
        out.w_down_grad[None],
        out.moe_in_grad,
        out.proj_grad,
        out.gate_b_grad.T,
        out.gate_c_grad.T,
        out.value_x_grad.T,
    )


def on_device(*args):
    routes = args[2].shape[1]
    experts, lane_count = lax.axis_size("sp"), lax.axis_size("tp")
    if experts == CORES * GROUPS and routes == CORES and lane_count == 4:
        return on_device_paired(*args)
    return on_device_general(*args)


def solution(mesh):
    in_specs = (
        P("sp", None),
        P("sp", None),
        P("sp", None),
        P("sp", None),
        P("sp", "tp", None),
        P("sp", "tp", None),
        P("sp", "tp", None),
        P("tp", "sp"),
        P("tp", "sp"),
        P("tp", "sp"),
        P(None, "tp"),
        P("tp", None),
    )
    out_specs = (
        P("sp", "tp", None),
        P("sp", "tp", None),
        P("sp", "tp", None),
        P("sp", "tp"),
        P("tp", "sp"),
        P("tp", "sp"),
        P("tp", "sp"),
        P("tp", "sp"),
    )
    return jax.shard_map(
        on_device, mesh=mesh, in_specs=in_specs, out_specs=out_specs, check_vma=False
    )
```

```python
import functools
import types

import jax
import jax.numpy as jnp
from jax import lax
from jax.experimental import pallas as pl
from jax.experimental.pallas import tpu as pltpu
from jax.sharding import PartitionSpec as P

TAPS = 3
GROUPS = 4
CORES = 2
MESH = pl.DeviceIdType.MESH


def place():
    s, t = lax.axis_index("sp"), lax.axis_index("tp")
    z, c = lax.div(s, CORES), lax.rem(s, CORES)
    x, y = lax.rem(t, 2), lax.div(t, 2)
    lanes = (t + 1 - 2 * x, t + 2 - 4 * y, 3 - t)
    return s, t, z, c, lanes


def span(index, width):
    return pl.ds(pl.multiple_of(index * width, width), width)


def remote(src, dst, send_sem, recv_sem, target):
    return pltpu.make_async_remote_copy(
        src_ref=src,
        dst_ref=dst,
        send_sem=send_sem,
        recv_sem=recv_sem,
        device_id=target,
        device_id_type=MESH,
    )


def half(quarter, side, width):
    return pl.ds(pl.multiple_of(quarter * width + side * (width // 2), width // 2), width // 2)


def from_behind(array, axis, by):
    count = lax.axis_size(axis)
    pairs = [(i, i + by) for i in range(count) if 0 <= i + by < count]
    return lax.ppermute(array, axis, pairs)


def on_device_general(
    moe_in,
    cotangent,
    routing,
    route_weight,
    w_gate,
    w_up,
    w_down,
    gate_b,
    gate_c,
    value_x,
    conv_taps,
    out_proj,
):
    tok_rows = routing.shape[0]
    top_routes = routing.shape[1]
    experts = lax.axis_size("sp")
    lane_count = lax.axis_size("tp")
    model_width = moe_in.shape[1]
    capacity = top_routes * tok_rows // experts
    flat_routes = routing.reshape(-1)
    route_count = flat_routes.shape[0]
    one_hot = (flat_routes[:, None] == jnp.arange(experts, dtype=jnp.int32)[None, :]).astype(
        jnp.int32
    )
    slot_rank = jnp.sum(jnp.cumsum(one_hot, axis=0) * one_hot, axis=1) - 1
    slot_index = flat_routes * capacity + slot_rank
    source = (
        jnp.zeros((route_count,), jnp.int32)
        .at[slot_index]
        .set(jnp.arange(route_count, dtype=jnp.int32))
    )
    owner_token = source // top_routes
    scales = route_weight.reshape(-1)[source][:, None]
    col_width = model_width // lane_count
    col_start = lax.axis_index("tp") * col_width
    rows_part = lax.dynamic_slice_in_dim(moe_in, col_start, col_width, 1)[owner_token]
    cot_slice = lax.dynamic_slice_in_dim(cotangent, col_start, col_width, 1)[owner_token]
    cot_part = (scales * cot_slice.astype(jnp.float32)).astype(jnp.bfloat16)
    moved = (
        lax.all_to_all(rows_part, "sp", split_axis=0, concat_axis=0, tiled=True),
        lax.all_to_all(cot_part, "sp", split_axis=0, concat_axis=0, tiled=True),
    )
    arrived, arrived_cot = (
        lax.all_gather(moved[0], "tp", axis=1, tiled=True),
        lax.all_gather(moved[1], "tp", axis=1, tiled=True),
    )
    contract_model = (((1,), (1,)), ((), ()))
    over_rows = (((0,), (0,)), ((), ()))
    gate_pre = lax.dot_general(
        arrived, w_gate[0], contract_model, preferred_element_type=jnp.float32
    )
    up_pre = lax.dot_general(arrived, w_up[0], contract_model, preferred_element_type=jnp.float32)
    sigmoid_gate = jax.nn.sigmoid(gate_pre)
    hidden = (gate_pre * sigmoid_gate * up_pre).astype(jnp.bfloat16)
    hidden_grad = lax.dot_general(
        arrived_cot, w_down[0], contract_model, preferred_element_type=jnp.float32
    )
    gate_grad = (
        hidden_grad * up_pre * sigmoid_gate * (1.0 + gate_pre * (1.0 - sigmoid_gate))
    ).astype(jnp.bfloat16)
    up_grad = (hidden_grad * gate_pre * sigmoid_gate).astype(jnp.bfloat16)
    w_gate_grad = lax.dot_general(
        gate_grad, arrived, over_rows, preferred_element_type=jnp.float32
    ).astype(jnp.bfloat16)[None]
    w_up_grad = lax.dot_general(
        up_grad, arrived, over_rows, preferred_element_type=jnp.float32
    ).astype(jnp.bfloat16)[None]
    w_down_grad = lax.dot_general(
        hidden, arrived_cot, over_rows, preferred_element_type=jnp.float32
    ).astype(jnp.bfloat16)[None]
    partial_value = jnp.dot(gate_grad, w_gate[0], preferred_element_type=jnp.float32) + jnp.dot(
        up_grad, w_up[0], preferred_element_type=jnp.float32
    )
    partial_value = lax.optimization_barrier(partial_value.astype(jnp.bfloat16)).astype(jnp.float32)
    summed = lax.psum_scatter(
        partial_value.astype(jnp.bfloat16), "tp", scatter_dimension=1, tiled=True
    )
    returned = lax.all_to_all(summed, "sp", split_axis=0, concat_axis=0, tiled=True)
    per_route = returned[slot_index].astype(jnp.float32)
    moe_in_grad = jnp.sum(per_route.reshape(tok_rows, top_routes, -1), axis=1).astype(jnp.bfloat16)
    full_grad = lax.all_gather(moe_in_grad, "tp", axis=1, tiled=True)
    stream_grad = (cotangent.astype(jnp.float32) + full_grad.astype(jnp.float32)).astype(
        jnp.bfloat16
    )
    mixed_in = lax.optimization_barrier(
        (gate_c.astype(jnp.float32) * value_x.astype(jnp.float32)).astype(jnp.bfloat16)
    )
    earlier = from_behind(mixed_in[:, tok_rows - (TAPS - 1) :], "sp", 1)
    extended = jnp.concatenate([earlier, mixed_in], axis=1).astype(jnp.float32)
    conv_out = jnp.zeros(mixed_in.shape, jnp.float32)
    for tap in range(TAPS):
        conv_out = conv_out + conv_taps[tap][:, None] * extended[:, tap : tap + tok_rows]
    mixer_act = (gate_b.astype(jnp.float32) * conv_out).astype(jnp.bfloat16)
    act_grad = lax.dot_general(
        out_proj, stream_grad, contract_model, preferred_element_type=jnp.float32
    )
    proj_rows = lax.psum_scatter(
        lax.dot_general(
            stream_grad, mixer_act, (((0,), (1,)), ((), ())), preferred_element_type=jnp.float32
        ).astype(jnp.bfloat16),
        "sp",
        scatter_dimension=0,
        tiled=True,
    ).astype(jnp.float32)
    proj_grad = proj_rows.T
    gate_b_grad = (act_grad * conv_out).astype(jnp.bfloat16)
    conv_grad = act_grad * gate_b.astype(jnp.float32)
    later = from_behind(conv_grad[:, : TAPS - 1], "sp", -1)
    extended_grad = jnp.concatenate([conv_grad, later], axis=1)
    mixed_grad = jnp.zeros(conv_grad.shape, jnp.float32)
    for tap in range(TAPS):
        offset = TAPS - 1 - tap
        mixed_grad = (
            mixed_grad + conv_taps[tap][:, None] * extended_grad[:, offset : offset + tok_rows]
        )
    gate_c_grad = (mixed_grad * value_x.astype(jnp.float32)).astype(jnp.bfloat16)
    value_x_grad = (mixed_grad * gate_c.astype(jnp.float32)).astype(jnp.bfloat16)
    return (
        w_gate_grad,
        w_up_grad,
        w_down_grad,
        moe_in_grad,
        proj_grad,
        gate_b_grad,
        gate_c_grad,
        value_x_grad,
    )


def last_dims(lhs, rhs):
    return lax.dot_general(lhs, rhs, (((1,), (1,)), ((), ())), preferred_element_type=jnp.float32)


def first_dims(lhs, rhs):
    return lax.dot_general(lhs, rhs, (((0,), (0,)), ((), ())), preferred_element_type=jnp.float32)


def plain(lhs, rhs):
    return jnp.dot(lhs, rhs, preferred_element_type=jnp.float32)


def step_kernel(names, *refs):
    r = types.SimpleNamespace(**dict(zip(names, refs)))
    s, t, z, c, lanes = place()
    tokens, model = r.moe.shape
    chan = r.gate_b.shape[1]
    cap = tokens // GROUPS
    width = model // 4
    hid_rows = r.w_gate.shape[0]
    devices = CORES * GROUPS
    f32, b16 = jnp.float32, jnp.bfloat16
    far = [z, z + 1 - 2 * lax.rem(z, 2), 3 - z, z + 2 - 4 * lax.div(z, 2)]
    peer = [(CORES * far[d] + c, t) for d in range(GROUPS)]
    mate = (CORES * z + 1 - c, t)
    after, before = (lax.rem(s + 1, devices), t), (lax.rem(s + devices - 1, devices), t)
    side_z = lax.rem(z + GROUPS + 2 * c - 1, GROUPS)
    side = (CORES * side_z + 1 - c, t)
    lane = [(s, lanes[j]) for j in range(3)]
    mine = span(t, width)
    sub = width // 4
    mine_sub = span(t, sub)

    loads = {}
    order = ("routing", "route_weight", "moe", "cot", "gate_c", "value_x", "w_gate", "w_up", "w_down", "gate_b", "taps", "out_proj")
    for i, key in enumerate(order):
        loads[key] = pltpu.make_async_copy(getattr(r, key), getattr(r, "v_" + key), r.load.at[i])
        loads[key].start()
    targets = peer[1:] + [mate] + lane + [side]
    barrier = pltpu.get_barrier_semaphore()
    for target in targets:
        pl.semaphore_signal(barrier, inc=1, device_id=target, device_id_type=MESH)

    down = lax.broadcasted_iota(jnp.int32, (tokens, tokens), 0)
    along = lax.broadcasted_iota(jnp.int32, (tokens, tokens), 1)
    eye = down == along

    def column(row):
        return jnp.sum(jnp.where(eye, row, 0.0), axis=1, keepdims=True)

    loads["routing"].wait()
    lead = r.v_routing[0:1, :]
    group = lax.div(lead, CORES)
    low, high = lax.rem(group, 2), lax.div(group, 2)
    z_low, z_high = lax.rem(z, 2), lax.div(z, 2)
    odd, upper = low + z_low - 2 * low * z_low, high + z_high - 2 * high * z_high
    slot = (odd + upper - 2 * odd * upper) + 2 * upper
    slot = slot.astype(f32)
    earlier = (column(slot) == slot) & (down < along)
    rank = jnp.sum(jnp.where(earlier, 1.0, 0.0), axis=0, keepdims=True)
    at_row = slot * cap + rank
    at_col = column(at_row)
    select = (at_row == down.astype(f32)).astype(f32).astype(b16)
    r.pick[...] = select
    unselect = (at_col == along.astype(f32)).astype(f32).astype(b16)
    for a, key in enumerate(("moe", "cot")):
        loads[key].wait()
        for n in range(4):
            cols = slice(n * width, (n + 1) * width)
            r.rows[a, :, :, cols] = (
                plain(select, getattr(r, "v_" + key)[:, cols]).astype(b16).reshape(GROUPS, cap, width)
            )
    for a in range(2):
        r.land[a, 0, c] = r.rows[a, 0]
    pl.semaphore_wait(barrier, len(targets))

    steps = [(a, d) for d in range(1, GROUPS) for a in range(2)]
    copies = []

    def send(*args):
        copy = remote(*args)
        copy.start()
        copies.append(copy)
        return copy

    first, small = {}, {}
    for a, d in steps[:2]:
        first[a, d] = send(
            r.rows.at[a, d, :, mine],
            r.land.at[a, d, c, :, mine],
            r.sz.at[a, d - 1],
            r.rz.at[a, d - 1],
            peer[d],
        )
    fourth, small_mate = {}, {}
    for a in range(2):
        fourth[a, 0] = send(
            r.rows.at[a, 0], r.land.at[a, 0, c], r.sm.at[a, 0], r.rm.at[a, 0], mate
        )
    loads["route_weight"].wait()
    is_even = lax.rem(lead, CORES) == 0
    by_core = [
        column(jnp.where(is_even, r.v_route_weight[k : k + 1, :], r.v_route_weight[1 - k : 2 - k, :]))
        for k in range(CORES)
    ]
    lane_at = lax.broadcasted_iota(jnp.int32, (tokens, 128), 1).astype(f32)
    row_at = lax.broadcasted_iota(jnp.int32, (8, 128), 0)
    for d in range(GROUPS):
        hit = at_col == lane_at + float(d * cap)
        picked = [jnp.sum(jnp.where(hit, by_core[k], 0.0), axis=0, keepdims=True) for k in range(CORES)]
        r.weights[d] = jnp.where(row_at == 0, picked[0], picked[1])
    r.weight_in[0, c] = r.weights[0]
    for d in range(1, GROUPS):
        small[d] = send(r.weights.at[d], r.weight_in.at[d, c], r.sw.at[d - 1], r.rw.at[d - 1], peer[d])
    small_mate[0] = send(
        r.weights.at[0], r.weight_in.at[0, c], r.sv.at[0], r.rv.at[0], mate
    )
    loads["gate_c"].wait()
    loads["value_x"].wait()
    mixed = (r.v_gate_c[...].astype(f32) * r.v_value_x[...].astype(f32)).astype(b16).astype(f32)
    r.edge[...] = mixed[tokens - 8 :, :]
    halo = send(r.edge, r.edge_in, r.sh.at[0], r.rh.at[0], after)

    for a, d in steps[2:]:
        first[a, d] = send(
            r.rows.at[a, d, :, mine],
            r.land.at[a, d, c, :, mine],
            r.sz.at[a, d - 1],
            r.rz.at[a, d - 1],
            peer[d],
        )

    second, third = {}, {}

    def e1(a, d):
        first[a, d].wait_recv()
        block = r.land.at[a, d, c, :, mine]
        for j in range(2):
            second[a, d, j] = send(block, block, r.sx.at[a, d - 1, j], r.rx.at[a, d - 1, j], lane[j])

    def e2(a, d):
        for j in range(2):
            second[a, d, j].wait_recv()
        for j in range(2):
            block = r.land.at[a, d, c, :, half(lanes[1 - j], j, width)]
            third[a, d, j] = send(block, block, r.sy.at[a, d - 1, j], r.ry.at[a, d - 1, j], lane[j])

    def e3(a, d):
        for j in range(2):
            third[a, d, j].wait_recv()
        block = r.land.at[a, d, c]
        fourth[a, d] = send(block, block, r.sm.at[a, d], r.rm.at[a, d], mate)
        if a == 1:
            small[d].wait_recv()
            block = r.weight_in.at[d, c]
            small_mate[d] = send(block, block, r.sv.at[d], r.rv.at[d], mate)

    def e4(a, d):
        fourth[a, d].wait_recv()

    cap_down = lax.broadcasted_iota(jnp.int32, (cap, 128), 0)
    cap_along = lax.broadcasted_iota(jnp.int32, (cap, 128), 1)

    unit = lax.broadcasted_iota(jnp.int32, (256, 256), 0) == lax.broadcasted_iota(
        jnp.int32, (256, 256), 1
    )
    r.unit[...] = unit.astype(f32).astype(b16)
    turns = ("w_gate", "w_up", "w_down")

    def turn(i, first_tile, count):
        source, out = getattr(r, "v_" + turns[i]), r.turned
        for n in range(first_tile, first_tile + count):
            at = slice(n * 256, (n + 1) * 256)
            out[i, at, :] = last_dims(r.unit[...], source[:, at]).astype(b16)

    def forward(d):
        small_mate[d].wait_recv()
        for k in range(CORES):
            tile = r.weight_in[d, k]
            row = jnp.sum(jnp.where(row_at == c, tile, 0.0), axis=0, keepdims=True)
            scale = jnp.sum(jnp.where(cap_down == cap_along, row, 0.0), axis=1, keepdims=True)
            r.scaled[d, k] = (scale * r.land[1, d, k].astype(f32)).astype(b16)
        x = r.land[0, d].reshape(CORES * cap, model)
        y = r.scaled[d].reshape(CORES * cap, model)
        block = hid_rows // 2
        for n in range(2):
            hs = slice(n * block, (n + 1) * block)
            if d == 0:
                gate = last_dims(x, r.v_w_gate[hs, :])
                up = last_dims(x, r.v_w_up[hs, :])
                grad = last_dims(y, r.v_w_down[hs, :])
            else:
                gate = plain(x, r.turned[0, :, hs])
                up = plain(x, r.turned[1, :, hs])
                grad = plain(y, r.turned[2, :, hs])
            sig = jax.nn.sigmoid(gate)
            silu = gate * sig
            r.hidden[d, :, hs] = (silu * up).astype(b16)
            r.gate_grad[d, :, hs] = (grad * up * sig * (1.0 + gate * (1.0 - sig))).astype(b16)
            r.up_grad[d, :, hs] = (grad * silu).astype(b16)

    swap, across, hop, home, spread, relay = {}, {}, {}, {}, {}, {}
    piece, fan, pass_on = {}, {}, {}

    def backward(d):
        for n in range(4):
            cols = slice(n * width, (n + 1) * width)
            value = plain(r.gate_grad[d], r.v_w_gate[:, cols]) + plain(
                r.up_grad[d], r.v_w_up[:, cols]
            )
            value = value.astype(b16).reshape(CORES, cap, width)
            for q in range(4):
                at = q * width + n * sub
                r.part[d, :, :, at : at + sub] = value[:, :, q * sub : (q + 1) * sub]
        swap[d] = send(r.part.at[d, 1 - c], r.mate_in.at[d], r.sa.at[d], r.ra.at[d], mate)

    def reduce_start(d):
        swap[d].wait_recv()
        r.total[d] = (r.part[d, c].astype(f32) + r.mate_in[d].astype(f32)).astype(b16)
        for j in range(2):
            for i, target in enumerate((2, j)):
                across[d, j, 1 - i] = send(
                    r.total.at[d, :, half(lanes[target], j, width)],
                    r.lane_in.at[d, j, 1 - i],
                    r.sb.at[d, j, 1 - i],
                    r.rb.at[d, j, 1 - i],
                    lane[j],
                )

    def reduce_mid(d):
        for j in range(2):
            across[d, j, 1].wait_recv()
            value = r.total[d, :, half(lanes[1 - j], j, width)].astype(f32) + r.lane_in[d, j, 1].astype(f32)
            r.hop[d, j] = value.astype(b16)
            hop[d, j] = send(r.hop.at[d, j], r.hop_in.at[d, j], r.sg.at[d, j], r.rg.at[d, j], lane[1 - j])

    def direct(d):
        return (2, 0, 1) if d >= 3 else (0, 1)

    def spread_start(d):
        block = r.home.at[d, :, mine]
        for j in direct(d):
            spread[d, j] = send(block, block, r.sd.at[d, j], r.rd.at[d, j], lane[j])

    def reduce_end(d):
        for j in range(2):
            across[d, j, 0].wait_recv()
            hop[d, j].wait_recv()
            value = r.total[d, :, half(t, j, width)].astype(f32) + r.lane_in[d, j, 0].astype(f32)
            value = value + r.hop_in[d, j].astype(f32)
            r.done[d, :, j * (width // 2) : (j + 1) * (width // 2)] = value.astype(b16)
        if d > 0:
            home[d] = send(
                r.done.at[d], r.home.at[d, :, mine], r.sc.at[d - 1], r.rc.at[d - 1], peer[d]
            )
        for e in (3, 2, 1, 0):
            own = pl.ds(pl.multiple_of(far[e] * width + t * sub, sub), sub)
            value = r.land[1, d, c, :, own].astype(f32) + r.done[d, :, span(far[e], sub)].astype(f32)
            if e > 0:
                r.op_out[d, e - 1] = value.astype(b16)
                piece[d, e] = send(
                    r.op_out.at[d, e - 1],
                    r.op.at[e, d, :, mine_sub],
                    r.sp.at[d, e - 1],
                    r.rp.at[d, e - 1],
                    peer[e],
                )
            else:
                r.op[0, d, :, mine_sub] = value.astype(b16)
        if d == 0:
            r.home[0, :, mine] = r.done[0]
            spread_start(0)

    def fan_start(d):
        for e in range(1, GROUPS):
            piece[d, e].wait_recv()
        block = r.op.at[:, d, :, mine_sub]
        for j in direct(d):
            fan[d, j] = send(block, block, r.sq.at[d, j], r.rq.at[d, j], lane[j])

    def pass_start(d):
        if len(direct(d)) == 3:
            return
        for j in range(2):
            fan[d, j].wait_recv()
        for j in range(2):
            block = r.op.at[2 * j : 2 * j + 2, d, :, span(lanes[1 - j], sub)]
            pass_on[d, j] = send(block, block, r.so.at[d, j], r.ro.at[d, j], lane[j])

    def pass_end(d):
        if len(direct(d)) == 3:
            for j in range(3):
                fan[d, j].wait_recv()
            return
        for j in range(2):
            pass_on[d, j].wait_recv()

    def home_in(d):
        home[d].wait_recv()
        spread_start(d)

    def relay_start(d):
        if len(direct(d)) == 3:
            return
        for j in range(2):
            spread[d, j].wait_recv()
        for j in range(2):
            block = r.home.at[d, :, half(lanes[1 - j], j, width)]
            relay[d, j] = send(block, block, r.se.at[d, j], r.re.at[d, j], lane[j])

    def relay_end(d):
        if len(direct(d)) == 3:
            for j in range(3):
                spread[d, j].wait_recv()
            return
        for j in range(2):
            relay[d, j].wait_recv()

    sources = (("w_gate_grad", "gate_grad", 0), ("w_up_grad", "up_grad", 0), ("w_down_grad", "hidden", 1))

    def weight_grad(i, *tiles):
        out, left, a = sources[i]
        lhs = getattr(r, left)[...].reshape(GROUPS * CORES * cap, hid_rows)
        for n in tiles:
            cols = slice(n * width, (n + 1) * width)
            rhs = r.land[0, :, :, :, cols] if a == 0 else r.scaled[:, :, :, cols]
            getattr(r, out)[:, cols] = first_dims(lhs, rhs.reshape(GROUPS * CORES * cap, width)).astype(b16)

    token_at = lax.broadcasted_iota(jnp.int32, (tokens, chan), 0)

    def conv_forward():
        halo.wait_recv()
        loads["taps"].wait()
        loads["gate_b"].wait()
        keep = jnp.where(s == 0, 0.0, 1.0)
        one, two = keep * r.edge_in[7:8, :], keep * r.edge_in[6:7, :]
        back_one = jnp.where(token_at == 0, one, pltpu.roll(mixed, 1, 0))
        back_two = jnp.where(
            token_at == 0, two, jnp.where(token_at == 1, one, pltpu.roll(mixed, 2, 0))
        )
        taps = r.v_taps
        conv = taps[0:1, :] * back_two + taps[1:2, :] * back_one + taps[2:3, :] * mixed
        r.conv[...] = conv
        act = (r.v_gate_b[...].astype(f32) * conv).astype(b16)
        r.act_in[0] = plain(r.pick[...], act).astype(b16).reshape(GROUPS, cap, chan)

    action = {}

    def act_start():
        for d in (3, 2, 1):
            action[d] = send(
                r.act_in.at[0], r.act_in.at[d], r.su.at[d - 1], r.ru.at[d - 1], peer[d]
            )

    def stream_of(pull, n):
        slabs = [r.home[:, :, q * width + n * sub : q * width + (n + 1) * sub] for q in range(4)]
        slab = jnp.concatenate(slabs, axis=2).reshape(tokens, width)
        return plain(pull, slab).astype(b16)

    last = {}

    def rim_start():
        for d in range(GROUPS):
            relay_end(d)
        loads["out_proj"].wait()
        for n in range(4):
            cols = slice(n * width, (n + 1) * width)
            full = stream_of(unselect[0:16, :], n)
            r.stream[0:16, cols] = (r.v_cot[0:16, cols].astype(f32) + full.astype(f32)).astype(b16)
        top = last_dims(r.stream[0:16, :], r.v_out_proj[...])[0:8, :]
        r.rim[...] = top * r.v_gate_b[0:16, :].astype(f32)[0:8, :]
        last[0] = send(r.rim, r.rim_in, r.sh.at[1], r.rh.at[1], before)

    def project():
        for d in range(1, GROUPS):
            action[d].wait_recv()
        for e in range(GROUPS):
            for d in range(GROUPS):
                r.mix[e, d] = r.act_in[e ^ d, d]
        for d in range(GROUPS):
            pass_end(d)
        narrow = width // CORES
        rows_all = GROUPS * GROUPS * cap
        mix = r.mix[...].reshape(rows_all, chan)
        there = r.op[:, :, :, span(1 - c, narrow)].reshape(rows_all, narrow)
        r.give[...] = first_dims(mix, there).astype(b16)
        last[1] = send(r.give, r.take, r.sn.at[0], r.rn.at[0], mate)
        here = r.op[:, :, :, span(c, narrow)].reshape(rows_all, narrow)
        r.proj_grad[...] = first_dims(mix, here)

    def stream_all():
        for n in range(4):
            cols = slice(n * width, (n + 1) * width)
            full = stream_of(unselect, n)
            r.full[:, cols] = full
            r.stream[:, cols] = (r.v_cot[:, cols].astype(f32) + full.astype(f32)).astype(b16)

    loads["w_gate"].wait()
    loads["w_up"].wait()
    loads["w_down"].wait()
    turn(2, 0, 2)
    e4(0, 0)
    e4(1, 0)
    forward(0)
    e1(*steps[0])
    conv_forward()
    e1(*steps[1])
    backward(0)
    turn(1, 2, 2)
    e1(*steps[2])
    turn(0, 4, 2)
    e1(*steps[3])
    turn(1, 0, 2)
    turn(0, 2, 2)
    e2(*steps[1])
    e2(*steps[0])
    turn(2, 4, 2)
    turn(1, 4, 2)
    e2(*steps[2])
    e1(*steps[5])
    act_start()
    turn(1, 6, 2)
    e2(*steps[3])
    e1(*steps[4])
    reduce_start(0)
    e3(*steps[1])
    turn(0, 6, 2)
    e3(*steps[0])
    turn(2, 2, 2)
    turn(0, 0, 2)
    e3(*steps[2])
    turn(2, 6, 2)
    e4(0, 1)
    e4(1, 1)
    forward(1)
    e3(*steps[3])
    e2(*steps[5])
    backward(1)
    e2(*steps[4])
    reduce_mid(0)
    e4(0, 2)
    e4(1, 2)
    forward(2)
    backward(2)
    e3(*steps[5])
    reduce_start(1)
    e3(*steps[4])
    reduce_start(2)
    reduce_end(0)
    e4(0, 3)
    e4(1, 3)
    forward(3)
    reduce_mid(1)
    backward(3)
    reduce_mid(2)
    weight_grad(0, 3)
    reduce_start(3)
    fan_start(0)
    relay_start(0)
    reduce_end(1)
    weight_grad(1, 0)
    weight_grad(0, 0)
    reduce_end(2)
    weight_grad(1, 1)
    reduce_mid(3)
    home_in(1)
    pass_start(0)
    weight_grad(2, 2)
    weight_grad(2, 1)
    fan_start(1)
    reduce_end(3)
    home_in(2)
    fan_start(2)
    pass_start(1)
    relay_start(1)
    relay_start(2)
    home_in(3)
    weight_grad(1, 2)
    weight_grad(2, 0)
    weight_grad(2, 3)
    fan_start(3)
    pass_start(2)
    weight_grad(0, 2)
    pass_start(3)
    weight_grad(1, 3)
    relay_start(3)
    weight_grad(0, 1)
    rim_start()
    stream_all()
    project()
    act_grad = last_dims(r.stream[...], r.v_out_proj[...])
    conv_grad = act_grad * r.v_gate_b[...].astype(f32)
    r.moe_in_grad[...] = r.full[:, mine]
    r.gate_b_grad[...] = (act_grad * r.conv[...]).astype(b16)
    last[0].wait_recv()
    keep = jnp.where(s == devices - 1, 0.0, 1.0)
    one, two = keep * r.rim_in[0:1, :], keep * r.rim_in[1:2, :]
    next_one = jnp.where(token_at == tokens - 1, one, pltpu.roll(conv_grad, tokens - 1, 0))
    next_two = jnp.where(
        token_at == tokens - 1,
        two,
        jnp.where(token_at == tokens - 2, one, pltpu.roll(conv_grad, tokens - 2, 0)),
    )
    taps = r.v_taps
    mixed_grad = taps[0:1, :] * next_two + taps[1:2, :] * next_one + taps[2:3, :] * conv_grad
    r.gate_c_grad[...] = (mixed_grad * r.v_value_x[...].astype(f32)).astype(b16)
    r.value_x_grad[...] = (mixed_grad * r.v_gate_c[...].astype(f32)).astype(b16)
    last[1].wait_recv()
    r.proj_grad[...] = r.proj_grad[...] + r.take[...].astype(f32)
    for copy in copies:
        copy.wait_send()


def store_kernel(*refs):
    count = len(refs) // 2
    copies = [pltpu.make_async_copy(refs[i], refs[count + i], refs[-1].at[i]) for i in range(count)]
    for copy in copies:
        copy.start()
    for copy in copies:
        copy.wait()


def on_device_paired(
    moe_in, cotangent, routing, route_weight, w_gate, w_up, w_down, gate_b, gate_c, value_x, conv_taps, out_proj
):
    tokens, model = moe_in.shape
    hid_rows = w_gate.shape[1]
    chan = gate_b.shape[0]
    cap, width = tokens // GROUPS, model // 4
    b16, f32 = moe_in.dtype, jnp.float32
    vmem, hbm = pl.BlockSpec(memory_space=pltpu.VMEM), pl.BlockSpec(memory_space=pltpu.HBM)
    dma = pltpu.SemaphoreType.DMA
    inputs = dict(
        routing=routing.T,
        route_weight=route_weight.T,
        moe=moe_in,
        cot=cotangent,
        w_gate=w_gate[0],
        w_up=w_up[0],
        w_down=w_down[0],
        gate_b=gate_b.T,
        gate_c=gate_c.T,
        value_x=value_x.T,
        taps=conv_taps,
        out_proj=out_proj,
    )
    outputs = dict(
        w_gate_grad=((hid_rows, model), b16),
        w_up_grad=((hid_rows, model), b16),
        w_down_grad=((hid_rows, model), b16),
        moe_in_grad=((tokens, width), b16),
        proj_grad=((chan, width // CORES), f32),
        gate_b_grad=((tokens, chan), b16),
        gate_c_grad=((tokens, chan), b16),
        value_x_grad=((tokens, chan), b16),
    )
    loaded = list(inputs)
    scratch = {"v_" + key: pltpu.VMEM(inputs[key].shape, inputs[key].dtype) for key in loaded}
    three, pair = GROUPS - 1, CORES * cap
    scratch |= dict(
        weights=pltpu.VMEM((GROUPS, 8, 128), f32),
        weight_in=pltpu.VMEM((GROUPS, CORES, 8, 128), f32),
        rows=pltpu.VMEM((2, GROUPS, cap, model), b16),
        land=pltpu.VMEM((2, GROUPS, CORES, cap, model), b16),
        scaled=pltpu.VMEM((GROUPS, CORES, cap, model), b16),
        hidden=pltpu.VMEM((GROUPS, pair, hid_rows), b16),
        gate_grad=pltpu.VMEM((GROUPS, pair, hid_rows), b16),
        up_grad=pltpu.VMEM((GROUPS, pair, hid_rows), b16),
        part=pltpu.VMEM((GROUPS, CORES, cap, model), b16),
        mate_in=pltpu.VMEM((GROUPS, cap, model), b16),
        total=pltpu.VMEM((GROUPS, cap, model), b16),
        lane_in=pltpu.VMEM((GROUPS, 2, 2, cap, width // 2), b16),
        done=pltpu.VMEM((GROUPS, cap, width), b16),
        home=pltpu.VMEM((GROUPS, cap, model), b16),
        full=pltpu.VMEM((tokens, model), b16),
        stream=pltpu.VMEM((tokens, model), b16),
        conv=pltpu.VMEM((tokens, chan), f32),
        edge=pltpu.VMEM((8, chan), f32),
        edge_in=pltpu.VMEM((8, chan), f32),
        rim=pltpu.VMEM((8, chan), f32),
        rim_in=pltpu.VMEM((8, chan), f32),
        give=pltpu.VMEM((chan, width // CORES), b16),
        take=pltpu.VMEM((chan, width // CORES), b16),
        unit=pltpu.VMEM((256, 256), b16),
        turned=pltpu.VMEM((3, model, hid_rows), b16),
        pick=pltpu.VMEM((tokens, tokens), b16),
        hop=pltpu.VMEM((GROUPS, 2, cap, width // 2), b16),
        hop_in=pltpu.VMEM((GROUPS, 2, cap, width // 2), b16),
        op=pltpu.VMEM((GROUPS, GROUPS, cap, width), b16),
        op_out=pltpu.VMEM((GROUPS, three, cap, width // 4), b16),
        act_in=pltpu.VMEM((GROUPS, GROUPS, cap, chan), b16),
        mix=pltpu.VMEM((GROUPS, GROUPS, cap, chan), b16),
        load=dma((len(loaded),)),
    )
    counts = dict(
        z=(2, three),
        w=(three,),
        x=(2, three, 2),
        y=(2, three, 2),
        m=(2, GROUPS),
        v=(GROUPS,),
        h=(2,),
        a=(GROUPS,),
        b=(GROUPS, 2, 2),
        g=(GROUPS, 2),
        c=(three,),
        d=(GROUPS, 3),
        e=(GROUPS, 2),
        p=(GROUPS, three),
        q=(GROUPS, 3),
        o=(GROUPS, 2),
        u=(three,),
        n=(1,),
    )
    for key, shape in counts.items():
        scratch["s" + key] = dma(shape)
        scratch["r" + key] = dma(shape)
    names = list(inputs) + list(outputs) + list(scratch)
    out = pl.pallas_call(
        functools.partial(step_kernel, names),
        out_shape=tuple(pltpu.VMEM(*shape) for shape in outputs.values()),
        in_specs=[hbm] * len(inputs),
        out_specs=(vmem,) * len(outputs),
        scratch_shapes=list(scratch.values()),
        compiler_params=pltpu.CompilerParams(
            collective_id=0, has_side_effects=True, vmem_limit_bytes=54 * 1024 * 1024
        ),
        name="step",
    )(*inputs.values())
    out = pl.pallas_call(
        store_kernel,
        out_shape=tuple(jax.ShapeDtypeStruct(*shape) for shape in outputs.values()),
        in_specs=[vmem] * len(outputs),
        out_specs=(hbm,) * len(outputs),
        scratch_shapes=[dma((len(outputs),))],
        compiler_params=pltpu.CompilerParams(vmem_limit_bytes=4 * 1024 * 1024),
        name="store",
    )(*out)
    out = types.SimpleNamespace(**dict(zip(outputs, out)))
    return (
        out.w_gate_grad[None],
        out.w_up_grad[None],
        out.w_down_grad[None],
        out.moe_in_grad,
        out.proj_grad,
        out.gate_b_grad.T,
        out.gate_c_grad.T,
        out.value_x_grad.T,
    )


def on_device(*args):
    routes = args[2].shape[1]
    experts, lane_count = lax.axis_size("sp"), lax.axis_size("tp")
    if experts == CORES * GROUPS and routes == CORES and lane_count == 4:
        return on_device_paired(*args)
    return on_device_general(*args)


def solution(mesh):
    in_specs = (
        P("sp", None),
        P("sp", None),
        P("sp", None),
        P("sp", None),
        P("sp", "tp", None),
        P("sp", "tp", None),
        P("sp", "tp", None),
        P("tp", "sp"),
        P("tp", "sp"),
        P("tp", "sp"),
        P(None, "tp"),
        P("tp", None),
    )
    out_specs = (
        P("sp", "tp", None),
        P("sp", "tp", None),
        P("sp", "tp", None),
        P("sp", "tp"),
        P("tp", "sp"),
        P("tp", "sp"),
        P("tp", "sp"),
        P("tp", "sp"),
    )
    return jax.shard_map(
        on_device, mesh=mesh, in_specs=in_specs, out_specs=out_specs, check_vma=False
    )
```
